32 devices in a mesh: gr: 2 (over x), fs: 8 (over z, y), tp: 2 (over core).
Axes of the slice: x: 2, y: 2, z: 4, core: 2. Of those that a mesh axis runs over, the one named last changes fastest.
Arguments:
- tokens: bfloat16 [4096, 2048], P(('gr', 'tp'), 'fs'), may hold values from -400 to 400
- norm_gain: float32 [2048], P('fs'), may hold values from 0.1 to 1.9
- up_weight: float32 [2048, 8192], P('fs', ('gr', 'tp')), may hold values from -0.125 to 0.125
- down_weight: float32 [8192, 2048], P('fs', ('gr', 'tp')), may hold values from -0.09375 to 0.09375
Outputs:
- mixed: bfloat16 [2048, 4096], P('fs', ('gr', 'tp'))
- up_ready: bfloat16 [2048, 8192], P(None, 'fs')
- down_ready: bfloat16 [8192, 2048], P('fs')
The draws below stay inside these ranges and needn't reach their ends.
All inputs are finite; a program needn't handle non-finite values.
Results may differ from the reference program's by a relative error of at most 0.023.
Values may be sent and summed in bfloat16 or wider, within the bound.
A program may use at most 64 MiB of HBM per device.

```python
import math
import jax
import jax.numpy as jnp
from jax import lax

D = 2048
FF = 8192
TOKENS = 4096
N_FS = 8


def draw_tokens(key, part):
    keys = jax.random.split(key, 3)
    row_scales = jnp.exp(jax.random.uniform(keys[0], (TOKENS, 1), jnp.float32) * math.log(10.0))
    column_scales = jnp.exp(jax.random.uniform(keys[1], (1, D), jnp.float32) * math.log(10.0))
    base = jax.random.truncated_normal(keys[2], -4.0, 4.0, (TOKENS, D), jnp.float32)
    return (base * row_scales * column_scales).astype(jnp.bfloat16)


def with_spikes(array, key, source, target, shards_of, factor):
    def block_of(axis_at):
        return (jnp.arange(array.shape[axis_at]) // (array.shape[axis_at] // shards_of)).reshape((-1,) + (1,) * (array.ndim - 1 - axis_at))

    one_side = jax.random.permutation(key, shards_of)[block_of(target)]
    other_side = (block_of(target) + shards_of // 2) % shards_of
    return jnp.where((block_of(source) == one_side) | (block_of(source) == other_side), factor * array, array)


def steps_of(own_key, shape, shards, least, largest):
    def one(position, parts):
        draws = jax.random.uniform(jax.random.fold_in(jax.random.fold_in(own_key, 6), position), (parts,), jnp.float32, least / len(shards), largest / len(shards))
        return jnp.repeat(jnp.exp(draws), shape[position] // parts).reshape((-1,) + (1,) * (len(shape) - position - 1))

    factor_of = one(*shards[0])
    for cut in shards[1:]:
        factor_of = factor_of * one(*cut)
    return factor_of


def scatter_about(stream_key, shape, scale, most, pieces=(), kind=jnp.bfloat16):
    drawn = jax.random.normal(stream_key, shape, jnp.float32) * scale
    if len(pieces) > 0:
        drawn = steps_of(stream_key, shape, pieces, -0.22, 0.18) * drawn
    return jnp.clip(drawn, min=-most, max=most).astype(kind)


def gaussian_with(own_key, shape, scale, bound, cuts, heavy, kind=jnp.bfloat16):
    entries = scale * jax.random.normal(own_key, shape, jnp.float32)
    if cuts:
        entries = entries * steps_of(own_key, shape, cuts, -0.22, 0.18)
    return jnp.clip(with_spikes(entries, jax.random.fold_in(own_key, 3), *heavy), -bound, bound).astype(kind)


def setup_inputs(seed: int = 0) -> dict:
    arg_keys = jax.random.split(jax.random.key(seed), 5)
    return {
        "tokens": draw_tokens(jax.random.fold_in(arg_keys[4], 71), 0),
        "norm_gain": jnp.clip(1.0 + 0.18 * jax.random.normal(arg_keys[1], (D,), jnp.float32), 0.1, 1.9),
        "up_weight": scatter_about(arg_keys[2], (D, FF), D ** -0.5, 0.125, ((0, 8), (1, 4)), jnp.float32),
        "down_weight": gaussian_with(arg_keys[3], (FF, D), FF ** -0.5, 0.09375, ((0, 8), (1, 4)), (0, 1, 8, 2.0), jnp.float32),
    }


epsilon = 1e-06

def reference(tokens, norm_gain, up_weight, down_weight):
    up_ready = (norm_gain[:, None] * up_weight).astype(jnp.bfloat16)
    down_ready = down_weight.astype(jnp.bfloat16)
    raw_up = jnp.dot(tokens, up_ready, preferred_element_type=jnp.float32)
    widened = tokens.astype(jnp.float32)
    row_scale = lax.rsqrt(lax.optimization_barrier(jnp.mean(widened * widened, axis=1)) + epsilon)
    hidden = jnp.square(jax.nn.relu(raw_up * row_scale[:, None])).astype(jnp.bfloat16)
    block = FF // N_FS

    def add_block(running, index):
        start = (index * block).astype(jnp.int32)
        piece = lax.dynamic_slice_in_dim(hidden, start, block, 1)
        weight_rows = lax.dynamic_slice_in_dim(down_ready, start, block, 0)
        partial_value = jnp.dot(piece, weight_rows, preferred_element_type=jnp.float32).astype(jnp.bfloat16)
        partial_value = lax.optimization_barrier(partial_value).astype(jnp.float32)
        return (running + partial_value, None)
    running, _ = lax.scan(add_block, jnp.zeros((TOKENS, D), jnp.float32), jnp.arange(N_FS, dtype=jnp.int32))
    return (running.T.astype(jnp.bfloat16), up_ready, down_ready)
```

```python
import functools

import jax
import jax.numpy as jnp
from jax import lax
from jax.experimental import pallas as pl
from jax.experimental.pallas import tpu as pltpu
from jax.sharding import PartitionSpec as P

MESH = pl.DeviceIdType.MESH
epsilon = 1e-06


def line_shape(count):
    short = max(d for d in range(1, count + 1) if count % d == 0 and d * d <= count)
    return count // short, short


def chunks(total, size):
    return min(total, size)


def kernel(
    G, n, T, Z, Y, k, E, early, late, send_count,
    tok_ref, gain_ref, upw_ref, dnw_ref,
    mixed_ref, up_full, dn_full,
    upw_v, dnw_v, gain_v, gain_col, up_bf, xbuf, tok_full, hidden, part,
    ybuf, zup, zdn, zup_late, zdn_late, yfin,
    load_sem, hand, send_sem, tok_recv, x_recv, up_recv, dn_recv,
    y_recv, zu_recv, zd_recv, zul_recv, zdl_recv, yf_recv,
    y_send, zu_send, zd_send, zul_send, zdl_send,
):
    g, f, t = lax.axis_index("gr"), lax.axis_index("fs"), lax.axis_index("tp")
    z, y = f // Y, f % Y
    q = g * T + t
    rows = upw_v.shape[0]
    sub = rows // G
    unit = up_full.shape[1]
    dcols = dnw_v.shape[1]
    feat = part.shape[2]
    here = tok_full.shape[1]
    slab = here // E
    pending = []

    def fresh():
        assert len(pending) < send_count
        return send_sem.at[len(pending)]

    def send(src, dst, rsem, dev, cond=None):
        copy = pltpu.make_async_remote_copy(
            src_ref=src, dst_ref=dst, send_sem=fresh(), recv_sem=rsem, device_id=dev, device_id_type=MESH
        )
        if cond is None:
            copy.start()
        else:
            pl.when(cond)(copy.start)
        pending.append((cond, copy))

    def arrived(ref, sem, cond=None):
        wait = pltpu.make_async_copy(ref, ref, sem).wait
        if cond is None:
            wait()
        else:
            pl.when(cond)(wait)

    def tok(c, e):
        return tok_full.at[c, pl.ds(e * slab, slab)]

    loads = []
    for e in range(E):
        loads.append(pltpu.make_async_copy(tok_ref.at[pl.ds(e * slab, slab)], tok(f, e), tok_recv.at[f, e]))
    loads.append(pltpu.make_async_copy(gain_ref, gain_v, load_sem.at[0]))
    for h in range(G):
        r = pl.ds(h * sub, sub)
        loads.append(pltpu.make_async_copy(upw_ref.at[r], upw_v.at[r], load_sem.at[1 + h]))
    loads.append(pltpu.make_async_copy(dnw_ref, dnw_v, load_sem.at[1 + G]))

    barrier = pltpu.get_barrier_semaphore()
    below, above = z > 0, z < Z - 1
    line = below.astype(jnp.int32) + above.astype(jnp.int32)

    def greet(sem, wide):
        def tell(dev):
            pl.semaphore_signal(sem, inc=1, device_id=dev, device_id_type=MESH)

        pl.when(above)(lambda: tell((g, f + Y, t)))
        pl.when(below)(lambda: tell((g, f - Y, t)))
        for o in range(1, Y):
            tell((g, z * Y + (y + o) % Y, t))
        if wide:
            for o in range(1, G):
                tell(((g + o) % G, f, t))
            for o in range(1, T):
                tell((g, f, (t + o) % T))

    greet(barrier, True)
    for copy in loads:
        copy.start()
    pl.semaphore_wait(barrier, line + (Y - 1) + (G - 1) + (T - 1))

    rounds = Z - 1
    greeted = [0]

    def next_round():
        if greeted[0] < rounds:
            greet(hand.at[greeted[0]], False)
            greeted[0] += 1

    def round_over(i):
        if i < rounds:
            pl.semaphore_wait(hand.at[i], line + (Y - 1))

    next_round()

    for copy in loads[E:E + 1]:
        copy.wait()
    wide_gain = jnp.broadcast_to(gain_v[...], (128, rows))
    gain_col[...] = wide_gain.T

    step = chunks(sub, 32)

    def convert_up(h):
        @pl.loop(0, sub // step)
        def _(i):
            r = pl.ds(pl.multiple_of(h * sub + i * step, step), step)
            column = gain_col[r, 0:1]
            for j in range(k):
                up_bf[j, r, :] = (column * upw_v[r, pl.ds(j * unit, unit)]).astype(jnp.bfloat16)

    def piece(c, h):
        return up_full.at[pl.ds(pl.multiple_of(c * rows + h * sub, sub), sub)]

    def half(j, h):
        return up_bf.at[j, pl.ds(pl.multiple_of(h * sub, sub), sub)]

    def share_tokens(e):
        loads[e].wait()
        own = tok(f, e)
        for o in range(1, Y):
            send(own, own, tok_recv.at[f, e], (g, z * Y + (y + o) % Y, t))
        send(own, own, tok_recv.at[f, e], (g, f + Y, t), above)
        send(own, own, tok_recv.at[f, e], (g, f - Y, t), below)

    share_tokens(0)
    for h in range(G):
        loads[E + 1 + h].wait()
    for oh in range(1, G):
        h = (g + oh) % G
        convert_up(h)
        for j in range(k):
            send(half(j, h), xbuf.at[G - oh, j], x_recv.at[j, G - oh], (h, f, t))
    round_over(0)
    next_round()
    convert_up(g)
    for e in range(1, E):
        share_tokens(e)

    def to_owner(j, source_q, src):
        owner = source_q * k + j
        local = pltpu.make_async_copy(src, piece(f, g), up_recv.at[f, g])
        pl.when(owner == f)(local.start)
        send(src, piece(f, g), up_recv.at[f, g], (g, owner, t), owner != f)

    for i in range(1, rounds):
        round_over(i)
        next_round()
    for j in range(k):
        to_owner(j, q, half(j, g))

    star = (f // k) % T
    is_star = t == star

    def dn_block(index):
        return dn_full.at[:, pl.ds(pl.multiple_of(index * dcols, dcols), dcols)]

    deep = dnw_v.shape[0]
    dstep = chunks(deep, 64)
    loads[E + 1 + G].wait()

    @pl.loop(0, deep // dstep)
    def _(i):
        r = pl.ds(pl.multiple_of(i * dstep, dstep), dstep)
        dn_full[r, pl.ds(pl.multiple_of(q * dcols, dcols), dcols)] = dnw_v[r, :].astype(jnp.bfloat16)

    def down_across(cond):
        for o in range(1, G):
            send(dn_block(q), dn_block(q), dn_recv.at[q], ((g + o) % G, f, t), cond)

    for o in range(1, T):
        send(dn_block(q), dn_block(q), dn_recv.at[q], (g, f, (t + o) % T))

    def relay_direct(c, cond):
        ok = is_star & cond
        arrived(piece(c, g), up_recv.at[c, g], ok)
        for o in range(1, G):
            send(piece(c, g), piece(c, g), up_recv.at[c, g], ((g + o) % G, f, t), ok)
        for o in range(1, T):
            send(piece(c, g), piece(c, g), up_recv.at[c, g], (g, f, (t + o) % T), ok)

    def relay_far(c, cond):
        ok = is_star & cond
        for oh in range(1, G):
            h = (g + oh) % G
            arrived(piece(c, h), up_recv.at[c, h], ok)
            for o in range(1, T):
                send(piece(c, h), piece(c, h), up_recv.at[c, h], (g, f, (t + o) % T), ok)

    def on_tokens(c, e, cond, up, down, cross):
        arrived(tok(c, e), tok_recv.at[c, e], cond)
        if up is not None:
            send(tok(c, e), tok(c, e), tok_recv.at[c, e], (g, f + Y, t), up)
        if down is not None:
            send(tok(c, e), tok(c, e), tok_recv.at[c, e], (g, f - Y, t), down)
        if cross:
            for o in range(1, Y):
                send(tok(c, e), tok(c, e), tok_recv.at[c, e], (g, z * Y + (y + o) % Y, t), cond)

    def from_exchange():
        for og in range(1, G):
            for j in range(k):
                arrived(xbuf.at[og, j], x_recv.at[j, og])
                to_owner(j, ((g + og) % G) * T + t, xbuf.at[og, j])

    for e in early:
        for o in range(1, Y):
            on_tokens(z * Y + (y + o) % Y, e, None, above, below, False)

    def pieces_at(s):
        if s == 0:
            return [(z * Y + (y + o) % Y, True) for o in range(Y)]
        lower, upper = z - s >= 0, z + s < Z
        zl, zu = jnp.maximum(z - s, 0), jnp.minimum(z + s, Z - 1)
        found = []
        for o in range(Y):
            found.append((zl * Y + (y + o) % Y, lower))
            found.append((zu * Y + (y + o) % Y, upper))
        return found

    def tokens_at(s):
        lower, upper = z - s >= 0, z + s < Z
        zl, zu = jnp.maximum(z - s, 0), jnp.minimum(z + s, Z - 1)
        for e in range(E):
            if e in early:
                for o in range(Y):
                    y2 = (y + o) % Y
                    on_tokens(zl * Y + y2, e, lower, lower & above, None, False)
                    on_tokens(zu * Y + y2, e, upper, None, upper & below, False)
            else:
                on_tokens(zl * Y + y, e, lower, lower & above, None, True)
                on_tokens(zu * Y + y, e, upper, None, upper & below, True)

    earlier = []
    for s in range(1, Z + 1):
        if s < Z:
            tokens_at(s)
        if s == 1:
            from_exchange()
            down_across(jnp.logical_not(is_star))
        now = pieces_at(s - 1)
        for c, cond in now:
            relay_direct(c, cond)
        for c, cond in earlier:
            relay_far(c, cond)
        earlier = now
    down_across(is_star)
    for c, cond in earlier:
        relay_far(c, cond)

    @pl.when(jnp.logical_not(is_star))
    def _():
        @pl.loop(0, n)
        def _(c):
            for h in range(G):
                arrived(piece(c, h), up_recv.at[c, h])

    width = n * tok_full.shape[2]

    def span(e):
        return pl.ds(e * slab, slab)

    def layer1(e):
        r = span(e)
        if e not in early:
            for zc in range(Z):
                for o in range(1, Y):
                    c = zc * Y + (y + o) % Y
                    arrived(tok(c, e), tok_recv.at[c, e])
        blocks = [tok_full[c, r, :] for c in range(n)]
        squares = None
        for block in blocks:
            wide = block.astype(jnp.float32)
            total = jnp.sum(wide * wide, axis=1, keepdims=True)
            squares = total if squares is None else squares + total
        scale = lax.rsqrt(squares / width + epsilon)
        raw = jnp.dot(jnp.concatenate(blocks, axis=1), up_full[...], preferred_element_type=jnp.float32)
        hidden[r, :] = jnp.square(jnp.maximum(raw * scale, 0.0)).astype(jnp.bfloat16)

    groups = G if Z % G == 0 else 1
    per_group = Z // groups

    def order(gv, zv, group):
        first = ((gv + group) % groups) * per_group
        return sorted(range(first, first + per_group), key=lambda zd: (-abs(zd - zv), zd))

    def nth(group, i):
        value = jnp.int32(0)
        for gv in range(G):
            for zv in range(Z):
                picks = order(gv, zv, group)
                for o in range(per_group):
                    value = jnp.where((g == gv) & (z == zv) & (i == o), picks[o], value)
        return value

    def cross_copy(zd, o, e):
        y2 = (y + o) % Y
        return pltpu.make_async_remote_copy(
            src_ref=part.at[zd * Y + y2, span(e)], dst_ref=ybuf.at[zd, Y - o, span(e)], send_sem=y_send.at[zd, o, e],
            recv_sem=y_recv.at[zd, Y - o, e], device_id=(g, z * Y + y2, t), device_id_type=MESH,
        )

    def line_copy(zd, e, up):
        c = zd * Y + y
        if up:
            return pltpu.make_async_remote_copy(
                src_ref=part.at[c, span(e)], dst_ref=zup.at[zd, span(e)], send_sem=zu_send.at[zd, e],
                recv_sem=zu_recv.at[zd, e], device_id=(g, f + Y, t), device_id_type=MESH,
            )
        return pltpu.make_async_remote_copy(
            src_ref=part.at[c, span(e)], dst_ref=zdn.at[zd, span(e)], send_sem=zd_send.at[zd, e],
            recv_sem=zd_recv.at[zd, e], device_id=(g, f - Y, t), device_id_type=MESH,
        )

    def late_copy(zd, y2, e, up):
        at = late.index(e)
        here_in = pl.ds(at * slab, slab)
        if up:
            return pltpu.make_async_remote_copy(
                src_ref=part.at[zd * Y + y2, span(e)], dst_ref=zup_late.at[zd, y2, here_in],
                send_sem=zul_send.at[zd, y2, at], recv_sem=zul_recv.at[zd, y2, at],
                device_id=(g, f + Y, t), device_id_type=MESH,
            )
        return pltpu.make_async_remote_copy(
            src_ref=part.at[zd * Y + y2, span(e)], dst_ref=zdn_late.at[zd, y2, here_in],
            send_sem=zdl_send.at[zd, y2, at], recv_sem=zdl_recv.at[zd, y2, at],
            device_id=(g, f - Y, t), device_id_type=MESH,
        )

    def layer2(group, e):
        r = span(e)

        @pl.loop(0, per_group)
        def _(i):
            zd = nth(group, i)
            cols = dn_full[:, pl.ds(pl.multiple_of(zd * (Y * feat), Y * feat), Y * feat)]
            whole = jnp.dot(hidden[r, :], cols, preferred_element_type=jnp.float32).astype(jnp.bfloat16)
            for y2 in range(Y):
                part[zd * Y + y2, r, :] = whole[:, y2 * feat:(y2 + 1) * feat]
            if e not in late:
                for o in range(1, Y):
                    cross_copy(zd, o, e).start()

    rstep = chunks(slab, 32)
    fstep = chunks(slab, 128)

    def add_up(c, e, extras, final=False):
        size = fstep if final else rstep

        @pl.loop(0, slab // size)
        def _(i):
            r = pl.ds(pl.multiple_of(e * slab + i * size, size), size)
            total = part[c, r, :].astype(jnp.float32)
            for ref, base in extras:
                total = total + ref[pl.ds(pl.multiple_of(base + i * size, size), size), :].astype(jnp.float32)
            if final:
                mixed_ref[:, r] = total.T.astype(jnp.bfloat16)
            else:
                part[c, r, :] = total.astype(jnp.bfloat16)

    ends = [
        (jnp.bool_(True), False, False) if Z == 1 else (z == 0, False, True),
    ]
    if Z > 1:
        ends.append((z == Z - 1, True, False))
    if Z > 2:
        ends.append((below & above, True, True))

    def finish(e, low, high, crossed):
        for cond, has_low, has_high in ends:
            extras = list(crossed) + ([low] if has_low else []) + ([high] if has_high else [])

            @pl.when(cond)
            def _():
                add_up(z * Y + y, e, extras, True)

    def reduce_slab(group, e):
        @pl.loop(0, per_group)
        def _(i):
            zd = nth(group, i)
            c = zd * Y + y
            base = e * slab
            crossed = [(ybuf.at[zd, o], base) for o in range(1, Y)]
            low, high = (zup.at[zd], base), (zdn.at[zd], base)
            for o in range(1, Y):
                arrived(ybuf.at[zd, o, span(e)], y_recv.at[zd, o, e])
            arrived(zup.at[zd, span(e)], zu_recv.at[zd, e], (zd >= z) & below)
            arrived(zdn.at[zd, span(e)], zd_recv.at[zd, e], (zd <= z) & above)
            if crossed:
                pl.when(((zd > z) & (z == 0)) | ((zd < z) & (z == Z - 1)))(lambda: add_up(c, e, crossed))
            pl.when((zd > z) & below)(lambda: add_up(c, e, crossed + [low]))
            pl.when((zd < z) & above)(lambda: add_up(c, e, crossed + [high]))
            pl.when(zd > z)(lambda: line_copy(zd, e, True).start())
            pl.when(zd < z)(lambda: line_copy(zd, e, False).start())
            pl.when(zd == z)(lambda: finish(e, low, high, crossed))

    def final_cross(o, e):
        at = late.index(e)
        y2 = (y + o) % Y
        return pltpu.make_async_remote_copy(
            src_ref=part.at[z * Y + y2, span(e)], dst_ref=yfin.at[Y - o, pl.ds(at * slab, slab)],
            send_sem=yf_recv.at[1, o, at], recv_sem=yf_recv.at[0, Y - o, at],
            device_id=(g, z * Y + y2, t), device_id_type=MESH,
        )

    def reduce_late(group, e):
        at = late.index(e)
        base = at * slab
        inside = pl.ds(base, slab)

        @pl.loop(0, per_group)
        def _(i):
            zd = nth(group, i)
            for o in range(1, Y + 1):
                y2 = (y + o) % Y
                c = zd * Y + y2
                low, high = (zup_late.at[zd, y2], base), (zdn_late.at[zd, y2], base)
                arrived(zup_late.at[zd, y2, inside], zul_recv.at[zd, y2, at], (zd >= z) & below)
                arrived(zdn_late.at[zd, y2, inside], zdl_recv.at[zd, y2, at], (zd <= z) & above)
                own = zd == z if o < Y else jnp.bool_(False)
                pl.when((zd > z) & below)(lambda: add_up(c, e, [low]))
                pl.when((zd < z) & above)(lambda: add_up(c, e, [high]))
                if o < Y:
                    for cond, has_low, has_high in ends:
                        extras = ([low] if has_low else []) + ([high] if has_high else [])
                        if extras:
                            pl.when(own & cond)(lambda: add_up(c, e, extras))
                    pl.when(own)(lambda: final_cross(o, e).start())
                pl.when(zd > z)(lambda: late_copy(zd, y2, e, True).start())
                pl.when(zd < z)(lambda: late_copy(zd, y2, e, False).start())

    def finish_late(e):
        at = late.index(e)
        base = at * slab
        for o in range(1, Y):
            arrived(yfin.at[o, pl.ds(base, slab)], yf_recv.at[0, o, at])
        finish(e, (zup_late.at[z, y], base), (zdn_late.at[z, y], base), [(yfin.at[o], base) for o in range(1, Y)])

    slabs = list(late) + [e for e in range(E) if e not in late]

    def reduce_any(group, e):
        if e in late:
            reduce_late(group, e)
        else:
            reduce_slab(group, e)

    waiting = []
    for group in range(groups):
        gd = (g + group) % G
        if groups == 1:
            others = [((g + o) % G) * T + t for o in range(1, G)]
            mine = [((g + o) % G) * T + (t + ot) % T for o in range(G) for ot in range(1, T)]
        elif group == 0:
            others, mine = [], [g * T + (t + ot) % T for ot in range(1, T)]
        else:
            others, mine = [gd * T + t], [gd * T + (t + ot) % T for ot in range(1, T)]
        for index in others:
            arrived(dn_block(index), dn_recv.at[index])
            for ot in range(1, T):
                send(dn_block(index), dn_block(index), dn_recv.at[index], (g, f, (t + ot) % T))
        for count, e in enumerate(slabs):
            if group == 0:
                layer1(e)
            if count == 0:
                for index in mine:
                    arrived(dn_block(index), dn_recv.at[index])
            layer2(group, e)
            waiting.append((group, e))
            if len(waiting) > 1:
                reduce_any(*waiting.pop(0))
    for item in waiting:
        reduce_any(*item)
    for e in late:
        finish_late(e)

    for cond, copy in pending:
        if cond is None:
            copy.wait_send()
        else:
            pl.when(cond)(copy.wait_send)
    for e in range(E):
        for zd in range(Z):
            if e in late:
                for y2 in range(Y):
                    pl.when(zd > z)(late_copy(zd, y2, e, True).wait_send)
                    pl.when(zd < z)(late_copy(zd, y2, e, False).wait_send)
            else:
                for o in range(1, Y):
                    cross_copy(zd, o, e).wait_send()
                pl.when(zd > z)(line_copy(zd, e, True).wait_send)
                pl.when(zd < z)(line_copy(zd, e, False).wait_send)
    for e in late:
        for o in range(1, Y):
            final_cross(o, e).wait_send()


def shards(dims, tokens, norm_gain, up_weight, down_weight):
    G, n, T = dims
    Z, Y = line_shape(n)
    rows, cols = up_weight.shape
    here, w = tokens.shape
    deep, dcols = down_weight.shape
    unit = cols * G * T // n
    k = n // (G * T)
    E = 4 if here % 128 == 0 else 1
    early = (E - 1,) if Y == 2 and E > 1 else ()
    late = (0,) if Y == 2 and E > 1 else ()
    width = rows * n
    feat = dcols * G * T // n
    slab = here // E
    L = max(len(late), 1)
    sends = E * (Y + 1) + 2 * k * G + 2 * G + G * T + 2 * Z * Y * (E + 1) * 2 + 2 * Z * Y * G * T + 2 * Z * E * Y
    bf = jnp.bfloat16
    dma = pltpu.SemaphoreType.DMA
    vmem = pl.BlockSpec(memory_space=pltpu.VMEM)
    hbm = pl.BlockSpec(memory_space=pltpu.HBM)
    return pl.pallas_call(
        functools.partial(kernel, G, n, T, Z, Y, k, E, early, late, sends),
        out_shape=(
            pltpu.VMEM((feat, here), bf),
            pltpu.VMEM((width, unit), bf),
            pltpu.VMEM((deep, dcols * G * T), bf),
        ),
        in_specs=[hbm] * 4,
        out_specs=(vmem, vmem, vmem),
        scratch_shapes=[
            pltpu.VMEM((rows, cols), jnp.float32),
            pltpu.VMEM((deep, dcols), jnp.float32),
            pltpu.VMEM((1, rows), jnp.float32),
            pltpu.VMEM((rows, 128), jnp.float32),
            pltpu.VMEM((k, rows, unit), bf),
            pltpu.VMEM((G, k, rows // G, unit), bf),
            pltpu.VMEM((n, here, w), bf),
            pltpu.VMEM((here, unit), bf),
            pltpu.VMEM((n, here, feat), bf),
            pltpu.VMEM((Z, Y, here, feat), bf),
            pltpu.VMEM((Z, here, feat), bf),
            pltpu.VMEM((Z, here, feat), bf),
            pltpu.VMEM((Z, Y, L * slab, feat), bf),
            pltpu.VMEM((Z, Y, L * slab, feat), bf),
            pltpu.VMEM((Y, L * slab, feat), bf),
            dma((G + 2,)), pltpu.SemaphoreType.REGULAR((max(Z - 1, 1),)), dma((sends,)),
            dma((n, E)), dma((k, G)), dma((n, G)), dma((G * T,)),
            dma((Z, Y, E)), dma((Z, E)), dma((Z, E)), dma((Z, Y, L)), dma((Z, Y, L)), dma((2, Y, L)),
            dma((Z, Y, E)), dma((Z, E)), dma((Z, E)), dma((Z, Y, L)), dma((Z, Y, L)),
        ],
        compiler_params=pltpu.CompilerParams(
            collective_id=0, has_side_effects=True, vmem_limit_bytes=52 * 1024 * 1024
        ),
    )(tokens, norm_gain[None, :], up_weight, down_weight)


def solution(mesh):
    dims = (mesh.shape["gr"], mesh.shape["fs"], mesh.shape["tp"])
    in_specs = (P(("gr", "tp"), "fs"), P("fs"), P("fs", ("gr", "tp")), P("fs", ("gr", "tp")))
    out_specs = (P("fs", ("gr", "tp")), P(None, "fs"), P("fs", None))
    return jax.shard_map(
        functools.partial(shards, dims), mesh=mesh, in_specs=in_specs, out_specs=out_specs, check_vma=False
    )
```

```python
import functools

import jax
import jax.numpy as jnp
from jax import lax
from jax.experimental import pallas as pl
from jax.experimental.pallas import tpu as pltpu
from jax.sharding import PartitionSpec as P

MESH = pl.DeviceIdType.MESH
epsilon = 1e-06


def line_shape(count):
    short = max(d for d in range(1, count + 1) if count % d == 0 and d * d <= count)
    return count // short, short


def chunks(total, size):
    return min(total, size)


def plan(Z, E, k):
    steps = [("exchange",), ("share", 0), ("down",), ("down across",), ("greet", 0), ("convert",)]
    steps += [("greet", i) for i in range(1, Z)]
    steps += [("owned",), ("share", 1)]
    steps += [("pass", j) for j in range(k)] + [("share", e) for e in range(2, E)]
    steps += [("direct", 0)] + [("tokens", 1, e) for e in range(E)]
    steps += [("direct", 1)] + [("tokens", 2, e) for e in range(E)]
    steps += [("direct", 2)] + [("direct", 3)] + [("tokens", 3, e) for e in range(E)]
    steps += [("far", s) for s in range(Z)]
    return steps

def kernel(
    G, n, T, Z, Y, k, E, C, LAG, INNER, early, send_count,
    tok_ref, gain_ref, upw_ref, dnw_ref,
    mixed_ref, up_full, dn_full,
    upw_v, dnw_v, gain_v, gain_col, up_bf, xbuf, tok_full, hidden, part,
    ybuf, zup, zdn,
    load_sem, hand, send_sem, tok_recv, x_recv, up_recv, dn_recv,
    y_recv, zu_recv, zd_recv, dn_send, y_send, zu_send, zd_send,
):
    g, f, t = lax.axis_index("gr"), lax.axis_index("fs"), lax.axis_index("tp")
    z, y = f // Y, f % Y
    q = g * T + t
    rows = upw_v.shape[0]
    sub = rows // G
    unit = up_full.shape[1]
    dcols = dnw_v.shape[1]
    feat = part.shape[2]
    here = tok_full.shape[1]
    slab = here // E
    per = G * T // Z
    pending = []

    def nth(i):
        value = 0 * z
        for zv in range(Z):
            order = sorted(range(Z), key=lambda zd: (-abs(zd - zv), zd))
            for o in range(Z):
                value = jnp.where((z == zv) & (i == o), order[o], value)
        return value

    def fresh():
        assert len(pending) < send_count
        return send_sem.at[len(pending)]

    def send(src, dst, rsem, dev, cond=None):
        copy = pltpu.make_async_remote_copy(
            src_ref=src, dst_ref=dst, send_sem=fresh(), recv_sem=rsem, device_id=dev, device_id_type=MESH
        )
        if cond is None:
            copy.start()
        else:
            pl.when(cond)(copy.start)
        pending.append((cond, copy))

    def arrived(ref, sem, cond=None):
        wait = pltpu.make_async_copy(ref, ref, sem).wait
        if cond is None:
            wait()
        else:
            pl.when(cond)(wait)

    def tok(c, e):
        return tok_full.at[c, pl.ds(e * slab, slab)]

    loads = []
    for e in range(E):
        loads.append(pltpu.make_async_copy(tok_ref.at[pl.ds(e * slab, slab)], tok(f, e), tok_recv.at[f, e]))
    loads.append(pltpu.make_async_copy(gain_ref, gain_v, load_sem.at[0]))
    for h in range(G):
        r = pl.ds(h * sub, sub)
        loads.append(pltpu.make_async_copy(upw_ref.at[r], upw_v.at[r], load_sem.at[1 + h]))
    loads.append(pltpu.make_async_copy(dnw_ref, dnw_v, load_sem.at[1 + G]))

    barrier = pltpu.get_barrier_semaphore()
    below, above = z > 0, z < Z - 1
    line = below.astype(jnp.int32) + above.astype(jnp.int32)

    def greet(sem, wide):
        def tell(dev):
            pl.semaphore_signal(sem, inc=1, device_id=dev, device_id_type=MESH)

        pl.when(above)(lambda: tell((g, f + Y, t)))
        pl.when(below)(lambda: tell((g, f - Y, t)))
        for o in range(1, Y):
            tell((g, z * Y + (y + o) % Y, t))
        if wide:
            for o in range(1, G):
                tell(((g + o) % G, f, t))
            for o in range(1, T):
                tell((g, f, (t + o) % T))

    greet(barrier, True)
    for copy in loads:
        copy.start()
    pl.semaphore_wait(barrier, line + (Y - 1) + (G - 1) + (T - 1))

    rounds = Z
    greeted = [0]

    def next_round():
        if greeted[0] < rounds:
            greet(hand.at[greeted[0]], False)
            greeted[0] += 1

    def round_over(i):
        if i < rounds:
            pl.semaphore_wait(hand.at[i], line + (Y - 1))

    next_round()

    for copy in loads[E:E + 1]:
        copy.wait()
    wide_gain = jnp.broadcast_to(gain_v[...], (128, rows))
    gain_col[...] = wide_gain.T

    step = chunks(sub, 32)

    def convert_up(h):
        @pl.loop(0, sub // step)
        def _(i):
            r = pl.ds(pl.multiple_of(h * sub + i * step, step), step)
            column = gain_col[r, 0:1]
            for j in range(k):
                up_bf[j, r, :] = (column * upw_v[r, pl.ds(j * unit, unit)]).astype(jnp.bfloat16)

    def piece(c, h):
        return up_full.at[pl.ds(pl.multiple_of(c * rows + h * sub, sub), sub)]

    def half(j, h):
        return up_bf.at[j, pl.ds(pl.multiple_of(h * sub, sub), sub)]

    def share_tokens(e):
        loads[e].wait()
        own = tok(f, e)
        for o in range(1, Y):
            send(own, own, tok_recv.at[f, e], (g, z * Y + (y + o) % Y, t))
        send(own, own, tok_recv.at[f, e], (g, f + Y, t), above)
        send(own, own, tok_recv.at[f, e], (g, f - Y, t), below)

    def start_exchange():
        for oh in range(1, G):
            h = (g + oh) % G
            convert_up(h)
            for j in range(k):
                send(half(j, h), xbuf.at[G - oh, j], x_recv.at[j, G - oh], (h, f, t))

    relay_core = f % T

    def to_owner(j, source_q, src):
        owner = source_q * k + j
        local = pltpu.make_async_copy(src, piece(f, g), up_recv.at[f, g])
        stays = (owner == f) & (relay_core == t)
        pl.when(stays)(local.start)
        send(src, piece(f, g), up_recv.at[f, g], (g, owner, relay_core), jnp.logical_not(stays))

    def start_owned():
        for j in range(k):
            to_owner(j, q, half(j, g))

    deep = dnw_v.shape[0]
    drows = deep // C

    def dn_block(index, i):
        return dn_full.at[pl.ds(i * drows, drows), pl.ds(pl.multiple_of(index * dcols, dcols), dcols)]

    dstep = chunks(deep, 64)

    def start_down():
        loads[E + 1 + G].wait()

        @pl.loop(0, deep // dstep)
        def _(i):
            r = pl.ds(pl.multiple_of(i * dstep, dstep), dstep)
            dn_full[r, pl.ds(pl.multiple_of(q * dcols, dcols), dcols)] = dnw_v[r, :].astype(jnp.bfloat16)

        for i in range(C):
            for o in range(1, T):
                send(dn_block(q, i), dn_block(q, i), dn_recv.at[q, i], (g, f, (t + o) % T))


    def down_across():
        for i in range(C):
            for o in range(1, G):
                send(dn_block(q, i), dn_block(q, i), dn_recv.at[q, i], ((g + o) % G, f, t))

    def relay_direct(c, cond):
        ok = (c % T == t) & cond
        arrived(piece(c, g), up_recv.at[c, g], ok)
        for o in range(1, G):
            send(piece(c, g), piece(c, g), up_recv.at[c, g], ((g + o) % G, f, t), ok)
        for o in range(1, T):
            send(piece(c, g), piece(c, g), up_recv.at[c, g], (g, f, (t + o) % T), ok)

    def relay_far(c, cond):
        ok = (c % T == t) & cond
        for oh in range(1, G):
            h = (g + oh) % G
            arrived(piece(c, h), up_recv.at[c, h], ok)
            for o in range(1, T):
                send(piece(c, h), piece(c, h), up_recv.at[c, h], (g, f, (t + o) % T), ok)

    def on_tokens(c, e, cond, up, down, cross):
        arrived(tok(c, e), tok_recv.at[c, e], cond)
        if up is not None:
            send(tok(c, e), tok(c, e), tok_recv.at[c, e], (g, f + Y, t), up)
        if down is not None:
            send(tok(c, e), tok(c, e), tok_recv.at[c, e], (g, f - Y, t), down)
        if cross:
            for o in range(1, Y):
                send(tok(c, e), tok(c, e), tok_recv.at[c, e], (g, z * Y + (y + o) % Y, t), cond)

    def from_exchange(j):
        for og in range(1, G):
            arrived(xbuf.at[og, j], x_recv.at[j, og])
            to_owner(j, ((g + og) % G) * T + t, xbuf.at[og, j])

    def pieces_at(s):
        if s == 0:
            return [(z * Y + (y + o) % Y, True) for o in range(Y)]
        lower, upper = z - s >= 0, z + s < Z
        zl, zu = jnp.maximum(z - s, 0), jnp.minimum(z + s, Z - 1)
        found = []
        for o in range(Y):
            found.append((zl * Y + (y + o) % Y, lower))
            found.append((zu * Y + (y + o) % Y, upper))
        return found

    def tokens_at(s, e):
        if s == 0:
            if e in early:
                for o in range(1, Y):
                    on_tokens(z * Y + (y + o) % Y, e, None, above, below, False)
            return
        lower, upper = z - s >= 0, z + s < Z
        zl, zu = jnp.maximum(z - s, 0), jnp.minimum(z + s, Z - 1)
        if e in early:
            for o in range(Y):
                y2 = (y + o) % Y
                on_tokens(zl * Y + y2, e, lower, lower & above, None, False)
                on_tokens(zu * Y + y2, e, upper, None, upper & below, False)
        else:
            on_tokens(zl * Y + y, e, lower, lower & above, None, True)
            on_tokens(zu * Y + y, e, upper, None, upper & below, True)

    def greet_round(i):
        round_over(i)
        next_round()

    def on_pieces(s, relay):
        for c, cond in pieces_at(s):
            relay(c, cond)

    for copy in loads[E + 1:E + 1 + G]:
        copy.wait()
    for step_name in plan(Z, E, k):
        kind, *at = step_name
        {
            "share": share_tokens, "exchange": start_exchange, "convert": lambda: convert_up(g), "greet": greet_round,
            "owned": start_owned, "pass": from_exchange, "tokens": tokens_at, "down": start_down,
            "down across": down_across,
            "direct": lambda s: on_pieces(s, relay_direct), "far": lambda s: on_pieces(s, relay_far),
        }[kind](*at)

    @pl.loop(0, n)
    def _(c):
        for h in range(G):
            arrived(piece(c, h), up_recv.at[c, h], c % T != t)

    width = n * tok_full.shape[2]

    def span(e):
        return pl.ds(pl.multiple_of(e * slab, slab), slab)

    def layer1(e):
        r = span(e)
        crossed_late = e >= 0
        for other in early:
            crossed_late = crossed_late & (e != other)

        @pl.when(crossed_late)
        def _():
            for zc in range(Z):
                for o in range(1, Y):
                    c = zc * Y + (y + o) % Y
                    arrived(tok_full.at[c, r], tok_recv.at[c, e])
        blocks = [tok_full[c, r, :] for c in range(n)]
        squares = None
        for block in blocks:
            wide = block.astype(jnp.float32)
            total = jnp.sum(wide * wide, axis=1, keepdims=True)
            squares = total if squares is None else squares + total
        scale = lax.rsqrt(squares / width + epsilon)
        raw = jnp.dot(jnp.concatenate(blocks, axis=1), up_full[...], preferred_element_type=jnp.float32)
        hidden[r, :] = jnp.square(jnp.maximum(raw * scale, 0.0)).astype(jnp.bfloat16)

    def cross_copy(zd, o, e):
        y2 = (y + o) % Y
        return pltpu.make_async_remote_copy(
            src_ref=part.at[zd * Y + y2, span(e)], dst_ref=ybuf.at[zd, Y - o, span(e)], send_sem=y_send.at[zd, o, e],
            recv_sem=y_recv.at[zd, Y - o, e], device_id=(g, z * Y + y2, t), device_id_type=MESH,
        )

    def line_copy(zd, e, up):
        c = zd * Y + y
        if up:
            return pltpu.make_async_remote_copy(
                src_ref=part.at[c, span(e)], dst_ref=zup.at[zd, span(e)], send_sem=zu_send.at[zd, e],
                recv_sem=zu_recv.at[zd, e], device_id=(g, f + Y, t), device_id_type=MESH,
            )
        return pltpu.make_async_remote_copy(
            src_ref=part.at[c, span(e)], dst_ref=zdn.at[zd, span(e)], send_sem=zd_send.at[zd, e],
            recv_sem=zd_recv.at[zd, e], device_id=(g, f - Y, t), device_id_type=MESH,
        )

    def layer2(i, e):
        r = span(e)
        zd = nth(i)
        cols = dn_full[:, pl.ds(pl.multiple_of(zd * (Y * feat), Y * feat), Y * feat)]
        whole = jnp.dot(hidden[r, :], cols, preferred_element_type=jnp.float32).astype(jnp.bfloat16)
        for y2 in range(Y):
            part[zd * Y + y2, r, :] = whole[:, y2 * feat:(y2 + 1) * feat]
        for o in range(1, Y):
            cross_copy(zd, o, e).start()

    rstep = chunks(slab, 32)
    fstep = chunks(slab, 128)

    def add_up(c, e, extras, final=False):
        size = fstep if final else rstep

        @pl.loop(0, slab // size)
        def _(i):
            r = pl.ds(pl.multiple_of(e * slab + i * size, size), size)
            total = part[c, r, :].astype(jnp.float32)
            for ref, base in extras:
                total = total + ref[pl.ds(pl.multiple_of(base + i * size, size), size), :].astype(jnp.float32)
            if final:
                mixed_ref[:, r] = total.T.astype(jnp.bfloat16)
            else:
                part[c, r, :] = total.astype(jnp.bfloat16)

    ends = [
        (jnp.bool_(True), False, False) if Z == 1 else (z == 0, False, True),
    ]
    if Z > 1:
        ends.append((z == Z - 1, True, False))
    if Z > 2:
        ends.append((below & above, True, True))

    def finish(e, low, high, crossed):
        for cond, has_low, has_high in ends:
            extras = list(crossed) + ([low] if has_low else []) + ([high] if has_high else [])

            @pl.when(cond)
            def _():
                add_up(z * Y + y, e, extras, True)

    def add_step(index):
        held = jnp.clip(index, 0, items - 1)
        zd, e = nth(held // E), held % E
        go = (index >= 0) & (index < items)
        going_up, going_down = go & (zd > z), go & (zd < z)
        c = zd * Y + y
        base = e * slab
        crossed = [(ybuf.at[zd, o], base) for o in range(1, Y)]
        low, high = (zup.at[zd], base), (zdn.at[zd], base)
        for o in range(1, Y):
            arrived(ybuf.at[zd, o, span(e)], y_recv.at[zd, o, e], go)
        arrived(zup.at[zd, span(e)], zu_recv.at[zd, e], go & (zd >= z) & below)
        arrived(zdn.at[zd, span(e)], zd_recv.at[zd, e], go & (zd <= z) & above)
        if crossed:
            pl.when((going_up & (z == 0)) | (going_down & (z == Z - 1)))(lambda: add_up(c, e, crossed))
        pl.when(going_up & below)(lambda: add_up(c, e, crossed + [low]))
        pl.when(going_down & above)(lambda: add_up(c, e, crossed + [high]))
        pl.when(going_up)(lambda: line_copy(zd, e, True).start())
        pl.when(going_down)(lambda: line_copy(zd, e, False).start())
        pl.when(go & (zd == z))(lambda: finish(e, low, high, crossed))

    def down_over(b, o, i):
        return pltpu.make_async_remote_copy(
            src_ref=dn_block(b, i), dst_ref=dn_block(b, i), send_sem=dn_send.at[b, o, i],
            recv_sem=dn_recv.at[b, i], device_id=(g, f, (t + o) % T), device_id_type=MESH,
        )

    def down_forward(i):
        zd = nth(i)
        for at in range(per):
            b = zd * per + at

            @pl.when((b // T != g) & (b % T == t))
            def _():
                for part_of in range(C):
                    arrived(dn_block(b, part_of), dn_recv.at[b, part_of])
                    for o in range(1, T):
                        down_over(b, o, part_of).start()

    def down_wait(i):
        zd = nth(i)
        for at in range(per):
            b = zd * per + at

            @pl.when(b % T != t)
            def _():
                for part_of in range(C):
                    arrived(dn_block(b, part_of), dn_recv.at[b, part_of])

    items = Z * E
    delay = LAG + jnp.where(below & above, INNER, 0)
    down_forward(0)

    @pl.loop(0, items + LAG + INNER)
    def _(stage):
        @pl.when(stage < items)
        def _():
            i, e = stage // E, stage % E
            pl.when(i == 0)(lambda: layer1(e))
            pl.when((e == E - 1) & (i < Z - 1))(lambda: down_forward(i + 1))
            pl.when(e == 0)(lambda: down_wait(i))
            layer2(i, e)

        add_step(stage - delay)

    for cond, copy in pending:
        if cond is None:
            copy.wait_send()
        else:
            pl.when(cond)(copy.wait_send)
    for e in range(E):
        for zd in range(Z):
            for o in range(1, Y):
                cross_copy(zd, o, e).wait_send()
            pl.when(zd > z)(line_copy(zd, e, True).wait_send)
            pl.when(zd < z)(line_copy(zd, e, False).wait_send)
    for b in range(G * T):
        for o in range(1, T):
            for i in range(C):
                pl.when((b // T != g) & (b % T == t))(down_over(b, o, i).wait_send)


def shards(dims, tokens, norm_gain, up_weight, down_weight):
    G, n, T = dims
    Z, Y = line_shape(n)
    rows, cols = up_weight.shape
    here, w = tokens.shape
    deep, dcols = down_weight.shape
    unit = cols * G * T // n
    k = n // (G * T)
    E = 4 if here % 128 == 0 else 1
    early = () if Y == 2 and E > 1 else ()
    C, LAG, INNER = 4, 2, 2
    width = rows * n
    feat = dcols * G * T // n
    sends = E * (Y + 1) + 2 * k * G + 2 * C * G * T + 2 * Z * Y * (E + 1) * 2 + 2 * Z * Y * G * T + 2 * Z * E * Y
    bf = jnp.bfloat16
    dma = pltpu.SemaphoreType.DMA
    vmem = pl.BlockSpec(memory_space=pltpu.VMEM)
    hbm = pl.BlockSpec(memory_space=pltpu.HBM)
    return pl.pallas_call(
        functools.partial(kernel, G, n, T, Z, Y, k, E, C, LAG, INNER, early, sends),
        out_shape=(
            pltpu.VMEM((feat, here), bf),
            pltpu.VMEM((width, unit), bf),
            pltpu.VMEM((deep, dcols * G * T), bf),
        ),
        in_specs=[hbm] * 4,
        out_specs=(vmem, vmem, vmem),
        scratch_shapes=[
            pltpu.VMEM((rows, cols), jnp.float32),
            pltpu.VMEM((deep, dcols), jnp.float32),
            pltpu.VMEM((1, rows), jnp.float32),
            pltpu.VMEM((rows, 128), jnp.float32),
            pltpu.VMEM((k, rows, unit), bf),
            pltpu.VMEM((G, k, rows // G, unit), bf),
            pltpu.VMEM((n, here, w), bf),
            pltpu.VMEM((here, unit), bf),
            pltpu.VMEM((n, here, feat), bf),
            pltpu.VMEM((Z, Y, here, feat), bf),
            pltpu.VMEM((Z, here, feat), bf),
            pltpu.VMEM((Z, here, feat), bf),
            dma((G + 2,)), pltpu.SemaphoreType.REGULAR((Z,)), dma((sends,)),
            dma((n, E)), dma((k, G)), dma((n, G)), dma((G * T, C)),
            dma((Z, Y, E)), dma((Z, E)), dma((Z, E)), dma((G * T, T, C)), dma((Z, Y, E)), dma((Z, E)), dma((Z, E)),
        ],
        compiler_params=pltpu.CompilerParams(
            collective_id=0, has_side_effects=True, vmem_limit_bytes=52 * 1024 * 1024
        ),
    )(tokens, norm_gain[None, :], up_weight, down_weight)


def solution(mesh):
    dims = (mesh.shape["gr"], mesh.shape["fs"], mesh.shape["tp"])
    in_specs = (P(("gr", "tp"), "fs"), P("fs"), P("fs", ("gr", "tp")), P("fs", ("gr", "tp")))
    out_specs = (P("fs", ("gr", "tp")), P(None, "fs"), P("fs", None))
    return jax.shard_map(
        functools.partial(shards, dims), mesh=mesh, in_specs=in_specs, out_specs=out_specs, check_vma=False
    )
```

```python
import functools

import jax
import jax.numpy as jnp
from jax import lax
from jax.experimental import pallas as pl
from jax.experimental.pallas import tpu as pltpu
from jax.sharding import PartitionSpec as P

MESH = pl.DeviceIdType.MESH
epsilon = 1e-06


def line_shape(count):
    short = max(d for d in range(1, count + 1) if count % d == 0 and d * d <= count)
    return count // short, short


def chunks(total, size):
    return min(total, size)


def plan(Z, B, k, S, C):
    early = C // 2
    steps = [("exchange",), ("share", 0), ("down",), ("down across", 0, C, True), ("down across", 0, early, False)]
    steps += [("greet", i) for i in range(Z)]
    steps += [("owned",)] + [("share", e) for e in range(1, B)]
    steps += [("pass", j, s) for s in range(S) for j in range(k)]
    for far in range(Z - 1):
        steps += [("direct", far, s) for s in range(S)]
        if far + 2 == Z:
            steps += [("direct", Z - 1, s) for s in range(S)] + [("down across", early, C, False)]
        steps += [("tokens", far + 1, e) for e in range(B)]
    steps += [("far", far, s) for s in range(S) for far in range(Z)]
    return steps


def kernel(
    G, n, T, Z, Y, k, E, B, S, C, LAG, INNER, send_count,
    tok_ref, gain_ref, upw_ref, dnw_ref,
    mixed_ref, up_full, dn_full,
    upw_v, dnw_v, gain_v, gain_col, up_bf, xbuf, tok_full, hidden, part,
    ybuf, zup, zdn,
    load_sem, hand, send_sem, tok_recv, x_recv, up_recv, dn_recv,
    y_recv, zu_recv, zd_recv, dn_send, y_send, zu_send, zd_send,
):
    g, f, t = lax.axis_index("gr"), lax.axis_index("fs"), lax.axis_index("tp")
    z, y = f // Y, f % Y
    q = g * T + t
    rows = upw_v.shape[0]
    sub = rows // G
    unit = up_full.shape[1]
    dcols = dnw_v.shape[1]
    feat = part.shape[2]
    here = tok_full.shape[1]
    slab = here // E
    batch = here // B
    per = G * T // Z
    pending = []

    def nth(i):
        value = 0 * z
        for zv in range(Z):
            order = sorted(range(Z), key=lambda zd: (-abs(zd - zv), zd))
            for o in range(Z):
                value = jnp.where((z == zv) & (i == o), order[o], value)
        return value

    def fresh():
        assert len(pending) < send_count
        return send_sem.at[len(pending)]

    def send(src, dst, rsem, dev, cond=None):
        copy = pltpu.make_async_remote_copy(
            src_ref=src, dst_ref=dst, send_sem=fresh(), recv_sem=rsem, device_id=dev, device_id_type=MESH
        )
        if cond is None:
            copy.start()
        else:
            pl.when(cond)(copy.start)
        pending.append((cond, copy))

    def arrived(ref, sem, cond=None):
        wait = pltpu.make_async_copy(ref, ref, sem).wait
        if cond is None:
            wait()
        else:
            pl.when(cond)(wait)

    def tok(c, e):
        return tok_full.at[c, pl.ds(e * batch, batch)]

    loads = []
    for e in range(B):
        loads.append(pltpu.make_async_copy(tok_ref.at[pl.ds(e * batch, batch)], tok(f, e), tok_recv.at[f, e]))
    loads.append(pltpu.make_async_copy(gain_ref, gain_v, load_sem.at[0]))
    for h in range(G):
        r = pl.ds(h * sub, sub)
        loads.append(pltpu.make_async_copy(upw_ref.at[r], upw_v.at[r], load_sem.at[1 + h]))
    loads.append(pltpu.make_async_copy(dnw_ref, dnw_v, load_sem.at[1 + G]))

    barrier = pltpu.get_barrier_semaphore()
    below, above = z > 0, z < Z - 1
    line = below.astype(jnp.int32) + above.astype(jnp.int32)

    def greet(sem, wide):
        def tell(dev):
            pl.semaphore_signal(sem, inc=1, device_id=dev, device_id_type=MESH)

        pl.when(above)(lambda: tell((g, f + Y, t)))
        pl.when(below)(lambda: tell((g, f - Y, t)))
        for o in range(1, Y):
            tell((g, z * Y + (y + o) % Y, t))
        if wide:
            for o in range(1, G):
                tell(((g + o) % G, f, t))
            for o in range(1, T):
                tell((g, f, (t + o) % T))

    for at in list(range(B, B + 1 + G)) + list(range(B)) + [B + 1 + G]:
        loads[at].start()
    greet(barrier, True)

    rounds = Z
    greeted = [0]

    def next_round():
        if greeted[0] < rounds:
            greet(hand.at[greeted[0]], False)
            greeted[0] += 1

    def round_over(i):
        if i < rounds:
            pl.semaphore_wait(hand.at[i], line + (Y - 1))

    loads[B].wait()
    wide_gain = jnp.broadcast_to(gain_v[...], (128, rows))
    gain_col[...] = wide_gain.T

    step = chunks(sub, 32)

    def convert_up(h):
        @pl.loop(0, sub // step)
        def _(i):
            r = pl.ds(pl.multiple_of(h * sub + i * step, step), step)
            column = gain_col[r, 0:1]
            for j in range(k):
                up_bf[j, r, :] = (column * upw_v[r, pl.ds(j * unit, unit)]).astype(jnp.bfloat16)

    bit = sub // S

    def piece(c, h, s):
        return up_full.at[pl.ds(pl.multiple_of(c * rows + h * sub + s * bit, bit), bit)]

    def half(j, h, s):
        return up_bf.at[j, pl.ds(pl.multiple_of(h * sub + s * bit, bit), bit)]

    def share_tokens(e):
        loads[e].wait()
        own = tok(f, e)
        for o in range(1, Y):
            send(own, own, tok_recv.at[f, e], (g, z * Y + (y + o) % Y, t))
        send(own, own, tok_recv.at[f, e], (g, f + Y, t), above)
        send(own, own, tok_recv.at[f, e], (g, f - Y, t), below)

    def xpart(og, j, s):
        return xbuf.at[og, j, pl.ds(s * bit, bit)]

    def start_exchange():
        for oh in range(1, G):
            h = (g + oh) % G
            for s in range(S):
                for j in range(k):
                    send(half(j, h, s), xpart(G - oh, j, s), x_recv.at[j, G - oh, s], (h, f, t))

    relay_core = f % T

    def to_owner(j, s, source_q, src):
        owner = source_q * k + j
        local = pltpu.make_async_copy(src, piece(f, g, s), up_recv.at[f, g, s])
        stays = (owner == f) & (relay_core == t)
        pl.when(stays)(local.start)
        send(src, piece(f, g, s), up_recv.at[f, g, s], (g, owner, relay_core), jnp.logical_not(stays))

    def start_owned():
        for s in range(S):
            for j in range(k):
                to_owner(j, s, q, half(j, g, s))

    deep = dnw_v.shape[0]
    drows = deep // C

    def dn_block(index, i):
        return dn_full.at[pl.ds(i * drows, drows), pl.ds(pl.multiple_of(index * dcols, dcols), dcols)]

    dstep = chunks(deep, 64)

    def start_down():
        loads[B + 1 + G].wait()

        @pl.loop(0, deep // dstep)
        def _(i):
            r = pl.ds(pl.multiple_of(i * dstep, dstep), dstep)
            dn_full[r, pl.ds(pl.multiple_of(q * dcols, dcols), dcols)] = dnw_v[r, :].astype(jnp.bfloat16)

        for i in range(C):
            for o in range(1, T):
                send(dn_block(q, i), dn_block(q, i), dn_recv.at[q, i], (g, f, (t + o) % T))


    def down_across(first, last, near=None):
        cond = None if near is None else ((nth(0) == q // per) == near)
        for i in range(first, last):
            for o in range(1, G):
                send(dn_block(q, i), dn_block(q, i), dn_recv.at[q, i], ((g + o) % G, f, t), cond)

    def relay_direct(c, s, cond):
        ok = (c % T == t) & cond
        arrived(piece(c, g, s), up_recv.at[c, g, s], ok)
        for o in range(1, G):
            send(piece(c, g, s), piece(c, g, s), up_recv.at[c, g, s], ((g + o) % G, f, t), ok)
        for o in range(1, T):
            send(piece(c, g, s), piece(c, g, s), up_recv.at[c, g, s], (g, f, (t + o) % T), ok)

    def relay_far(c, s, cond):
        ok = (c % T == t) & cond
        for oh in range(1, G):
            h = (g + oh) % G
            arrived(piece(c, h, s), up_recv.at[c, h, s], ok)
            for o in range(1, T):
                send(piece(c, h, s), piece(c, h, s), up_recv.at[c, h, s], (g, f, (t + o) % T), ok)

    def on_tokens(c, e, cond, up, down):
        arrived(tok(c, e), tok_recv.at[c, e], cond)
        if up is not None:
            send(tok(c, e), tok(c, e), tok_recv.at[c, e], (g, f + Y, t), up)
        if down is not None:
            send(tok(c, e), tok(c, e), tok_recv.at[c, e], (g, f - Y, t), down)
        for o in range(1, Y):
            send(tok(c, e), tok(c, e), tok_recv.at[c, e], (g, z * Y + (y + o) % Y, t), cond)

    def from_exchange(j, s):
        for og in range(1, G):
            arrived(xpart(og, j, s), x_recv.at[j, og, s])
            to_owner(j, s, ((g + og) % G) * T + t, xpart(og, j, s))

    def pieces_at(s):
        if s == 0:
            return [(z * Y + (y + o) % Y, True) for o in range(Y)]
        lower, upper = z - s >= 0, z + s < Z
        zl, zu = jnp.maximum(z - s, 0), jnp.minimum(z + s, Z - 1)
        found = []
        for o in range(Y):
            found.append((zl * Y + (y + o) % Y, lower))
            found.append((zu * Y + (y + o) % Y, upper))
        return found

    def tokens_at(s, e):
        lower, upper = z - s >= 0, z + s < Z
        zl, zu = jnp.maximum(z - s, 0), jnp.minimum(z + s, Z - 1)
        on_tokens(zl * Y + y, e, lower, lower & above, None)
        on_tokens(zu * Y + y, e, upper, None, upper & below)

    def greet_round(i):
        round_over(i)
        next_round()

    def on_pieces(far, s, relay):
        for c, cond in pieces_at(far):
            relay(c, s, cond)

    for copy in loads[B + 1:B + 1 + G]:
        copy.wait()
    for h in range(G):
        convert_up(h)
    pl.semaphore_wait(barrier, line + (Y - 1) + (G - 1) + (T - 1))
    next_round()
    for step_name in plan(Z, B, k, S, C):
        kind, *at = step_name
        {
            "share": share_tokens, "exchange": start_exchange, "greet": greet_round,
            "owned": start_owned, "pass": from_exchange, "tokens": tokens_at, "down": start_down,
            "down across": down_across,
            "direct": lambda far, s: on_pieces(far, s, relay_direct), "far": lambda far, s: on_pieces(far, s, relay_far),
        }[kind](*at)

    @pl.loop(0, n)
    def _(c):
        for h in range(G):
            for s in range(S):
                arrived(piece(c, h, s), up_recv.at[c, h, s], c % T != t)

    width = n * tok_full.shape[2]

    def span(e):
        return pl.ds(pl.multiple_of(e * slab, slab), slab)

    def layer1(e):
        r = span(e)
        @pl.when(e % (E // B) == 0)
        def _():
            for zc in range(Z):
                for o in range(1, Y):
                    c = zc * Y + (y + o) % Y
                    at = e // (E // B)
                    rows_in = pl.ds(pl.multiple_of(at * batch, batch), batch)
                    arrived(tok_full.at[c, rows_in], tok_recv.at[c, at])

        blocks = [tok_full[c, r, :] for c in range(n)]
        squares = None
        for block in blocks:
            wide = block.astype(jnp.float32)
            total = jnp.sum(wide * wide, axis=1, keepdims=True)
            squares = total if squares is None else squares + total
        scale = lax.rsqrt(squares / width + epsilon)
        raw = jnp.dot(jnp.concatenate(blocks, axis=1), up_full[...], preferred_element_type=jnp.float32)
        hidden[r, :] = jnp.square(jnp.maximum(raw * scale, 0.0)).astype(jnp.bfloat16)

    def cross_copy(zd, o, e):
        y2 = (y + o) % Y
        return pltpu.make_async_remote_copy(
            src_ref=part.at[zd * Y + y2, span(e)], dst_ref=ybuf.at[zd, Y - o, span(e)], send_sem=y_send.at[zd, o, e],
            recv_sem=y_recv.at[zd, Y - o, e], device_id=(g, z * Y + y2, t), device_id_type=MESH,
        )

    def line_copy(zd, e, up):
        c = zd * Y + y
        if up:
            return pltpu.make_async_remote_copy(
                src_ref=part.at[c, span(e)], dst_ref=zup.at[zd, span(e)], send_sem=zu_send.at[zd, e],
                recv_sem=zu_recv.at[zd, e], device_id=(g, f + Y, t), device_id_type=MESH,
            )
        return pltpu.make_async_remote_copy(
            src_ref=part.at[c, span(e)], dst_ref=zdn.at[zd, span(e)], send_sem=zd_send.at[zd, e],
            recv_sem=zd_recv.at[zd, e], device_id=(g, f - Y, t), device_id_type=MESH,
        )

    def layer2(i, e):
        r = span(e)
        zd = nth(i)
        cols = dn_full[:, pl.ds(pl.multiple_of(zd * (Y * feat), Y * feat), Y * feat)]
        whole = jnp.dot(hidden[r, :], cols, preferred_element_type=jnp.float32).astype(jnp.bfloat16)
        for y2 in range(Y):
            part[zd * Y + y2, r, :] = whole[:, y2 * feat:(y2 + 1) * feat]
        for o in range(1, Y):
            cross_copy(zd, o, e).start()

    rstep = chunks(slab, 32)
    fstep = chunks(slab, 128)

    def add_up(c, e, extras, final=False):
        size = fstep if final else rstep

        @pl.loop(0, slab // size)
        def _(i):
            r = pl.ds(pl.multiple_of(e * slab + i * size, size), size)
            total = part[c, r, :].astype(jnp.float32)
            for ref, base in extras:
                total = total + ref[pl.ds(pl.multiple_of(base + i * size, size), size), :].astype(jnp.float32)
            if final:
                mixed_ref[:, r] = total.T.astype(jnp.bfloat16)
            else:
                part[c, r, :] = total.astype(jnp.bfloat16)

    ends = [
        (jnp.bool_(True), False, False) if Z == 1 else (z == 0, False, True),
    ]
    if Z > 1:
        ends.append((z == Z - 1, True, False))
    if Z > 2:
        ends.append((below & above, True, True))

    def finish(e, low, high, crossed):
        for cond, has_low, has_high in ends:
            extras = list(crossed) + ([low] if has_low else []) + ([high] if has_high else [])

            @pl.when(cond)
            def _():
                add_up(z * Y + y, e, extras, True)

    def add_step(index):
        held = jnp.clip(index, 0, items - 1)
        zd, e = nth(held // E), held % E
        go = (index >= 0) & (index < items)
        going_up, going_down = go & (zd > z), go & (zd < z)
        c = zd * Y + y
        base = e * slab
        crossed = [(ybuf.at[zd, o], base) for o in range(1, Y)]
        low, high = (zup.at[zd], base), (zdn.at[zd], base)
        for o in range(1, Y):
            arrived(ybuf.at[zd, o, span(e)], y_recv.at[zd, o, e], go)
        arrived(zup.at[zd, span(e)], zu_recv.at[zd, e], go & (zd >= z) & below)
        arrived(zdn.at[zd, span(e)], zd_recv.at[zd, e], go & (zd <= z) & above)
        if crossed:
            pl.when((going_up & (z == 0)) | (going_down & (z == Z - 1)))(lambda: add_up(c, e, crossed))
        pl.when(going_up & below)(lambda: add_up(c, e, crossed + [low]))
        pl.when(going_down & above)(lambda: add_up(c, e, crossed + [high]))
        pl.when(going_up)(lambda: line_copy(zd, e, True).start())
        pl.when(going_down)(lambda: line_copy(zd, e, False).start())
        pl.when(go & (zd == z))(lambda: finish(e, low, high, crossed))

    def down_over(b, o, i):
        return pltpu.make_async_remote_copy(
            src_ref=dn_block(b, i), dst_ref=dn_block(b, i), send_sem=dn_send.at[b, o, i],
            recv_sem=dn_recv.at[b, i], device_id=(g, f, (t + o) % T), device_id_type=MESH,
        )

    def down_forward(i):
        zd = nth(i)
        for at in range(per):
            b = zd * per + at

            @pl.when((b // T != g) & (b % T == t))
            def _():
                for part_of in range(C):
                    arrived(dn_block(b, part_of), dn_recv.at[b, part_of])
                    for o in range(1, T):
                        down_over(b, o, part_of).start()

    def down_wait(i):
        zd = nth(i)
        for at in range(per):
            b = zd * per + at

            @pl.when(b % T != t)
            def _():
                for part_of in range(C):
                    arrived(dn_block(b, part_of), dn_recv.at[b, part_of])

    items = Z * E
    delay = LAG + jnp.where(below & above, INNER, 0)
    down_forward(0)

    @pl.loop(0, items + LAG + INNER)
    def _(stage):
        @pl.when(stage < items)
        def _():
            i, e = stage // E, stage % E
            pl.when(i == 0)(lambda: layer1(e))
            pl.when((e == E - 1) & (i < Z - 1))(lambda: down_forward(i + 1))
            pl.when(e == 0)(lambda: down_wait(i))
            layer2(i, e)

        add_step(stage - delay)

    for cond, copy in pending:
        if cond is None:
            copy.wait_send()
        else:
            pl.when(cond)(copy.wait_send)
    for e in range(E):
        for zd in range(Z):
            for o in range(1, Y):
                cross_copy(zd, o, e).wait_send()
            pl.when(zd > z)(line_copy(zd, e, True).wait_send)
            pl.when(zd < z)(line_copy(zd, e, False).wait_send)
    for b in range(G * T):
        for o in range(1, T):
            for i in range(C):
                pl.when((b // T != g) & (b % T == t))(down_over(b, o, i).wait_send)


def drain(cuts, mixed_in, up_in, dn_in, mixed_out, up_out, dn_out, sems):
    copies = []
    for at, (src, dst) in enumerate([(up_in, up_out), (dn_in, dn_out), (mixed_in, mixed_out)]):
        size = src.shape[0] // cuts
        for i in range(cuts):
            r = pl.ds(i * size, size)
            copies.append(pltpu.make_async_copy(src.at[r], dst.at[r], sems.at[at, i]))
    for copy in copies:
        copy.start()
    for copy in copies:
        copy.wait()


def shards(dims, tokens, norm_gain, up_weight, down_weight):
    G, n, T = dims
    Z, Y = line_shape(n)
    rows, cols = up_weight.shape
    here, w = tokens.shape
    deep, dcols = down_weight.shape
    unit = cols * G * T // n
    k = n // (G * T)
    E = 4 if here % 128 == 0 else 1
    B = 2 if E % 2 == 0 else 1
    S, C, LAG, INNER = 1, 4, 2, 2
    width = rows * n
    feat = dcols * G * T // n
    sends = B * (Y + 1) + 2 * (Z - 1) * B * Y
    sends += k * (G - 1) * S + k * G * S + C * (T - 1) + 2 * C * (G - 1)
    sends += (2 * Z - 1) * Y * S * ((G - 1) + G * (T - 1))
    bf = jnp.bfloat16
    dma = pltpu.SemaphoreType.DMA
    vmem = pl.BlockSpec(memory_space=pltpu.VMEM)
    hbm = pl.BlockSpec(memory_space=pltpu.HBM)
    held = pl.pallas_call(
        functools.partial(kernel, G, n, T, Z, Y, k, E, B, S, C, LAG, INNER, sends),
        out_shape=(
            pltpu.VMEM((feat, here), bf),
            pltpu.VMEM((width, unit), bf),
            pltpu.VMEM((deep, dcols * G * T), bf),
        ),
        in_specs=[hbm] * 4,
        out_specs=(vmem, vmem, vmem),
        scratch_shapes=[
            pltpu.VMEM((rows, cols), jnp.float32),
            pltpu.VMEM((deep, dcols), jnp.float32),
            pltpu.VMEM((1, rows), jnp.float32),
            pltpu.VMEM((rows, 128), jnp.float32),
            pltpu.VMEM((k, rows, unit), bf),
            pltpu.VMEM((G, k, rows // G, unit), bf),
            pltpu.VMEM((n, here, w), bf),
            pltpu.VMEM((here, unit), bf),
            pltpu.VMEM((n, here, feat), bf),
            pltpu.VMEM((Z, Y, here, feat), bf),
            pltpu.VMEM((Z, here, feat), bf),
            pltpu.VMEM((Z, here, feat), bf),
            dma((G + 2,)), pltpu.SemaphoreType.REGULAR((Z,)), dma((sends,)),
            dma((n, B)), dma((k, G, S)), dma((n, G, S)), dma((G * T, C)),
            dma((Z, Y, E)), dma((Z, E)), dma((Z, E)), dma((G * T, T, C)), dma((Z, Y, E)), dma((Z, E)), dma((Z, E)),
        ],
        compiler_params=pltpu.CompilerParams(
            collective_id=0, has_side_effects=True, vmem_limit_bytes=52 * 1024 * 1024
        ),
    )(tokens, norm_gain[None, :], up_weight, down_weight)
    cuts = 4
    return pl.pallas_call(
        functools.partial(drain, cuts),
        out_shape=tuple(jax.ShapeDtypeStruct(x.shape, bf) for x in held),
        in_specs=[vmem] * 3,
        out_specs=(hbm,) * 3,
        scratch_shapes=[dma((3, cuts))],
        compiler_params=pltpu.CompilerParams(vmem_limit_bytes=12 * 1024 * 1024),
    )(*held)


def solution(mesh):
    dims = (mesh.shape["gr"], mesh.shape["fs"], mesh.shape["tp"])
    in_specs = (P(("gr", "tp"), "fs"), P("fs"), P("fs", ("gr", "tp")), P("fs", ("gr", "tp")))
    out_specs = (P("fs", ("gr", "tp")), P(None, "fs"), P("fs", None))
    return jax.shard_map(
        functools.partial(shards, dims), mesh=mesh, in_specs=in_specs, out_specs=out_specs, check_vma=False
    )
```

```python
import functools

import jax
import jax.numpy as jnp
from jax import lax
from jax.experimental import pallas as pl
from jax.experimental.pallas import tpu as pltpu
from jax.sharding import PartitionSpec as P

MESH = pl.DeviceIdType.MESH
epsilon = 1e-06


def line_shape(count):
    short = max(d for d in range(1, count + 1) if count % d == 0 and d * d <= count)
    return count // short, short


def chunks(total, size):
    return min(total, size)


def plan(Z, B, k, S, C):
    early = C // 2
    steps = [("exchange",)] + [("share", e) for e in range(B)] + [("down",), ("down across", 0, C, True), ("down across", 0, early, False)]
    steps += [("greet",), ("owned",)]
    steps += [("pass", j, s) for s in range(S) for j in range(k)]
    for far in range(Z - 1):
        steps += [("direct", far, s) for s in range(S)]
        if far + 2 == Z:
            steps += [("direct", Z - 1, s) for s in range(S)] + [("down across", early, C, False)]
        steps += [("tokens", far + 1, e) for e in range(B)]
    steps += [("far", far, s) for s in range(S) for far in range(Z)]
    return steps


def kernel(
    G, n, T, Z, Y, k, E, B, S, C, LAG, INNER, send_count,
    tok_ref, gain_ref, upw_ref, dnw_ref,
    mixed_ref, up_full, dn_full,
    upw_v, dnw_v, gain_v, gain_col, up_bf, xbuf, tok_full, hidden, part,
    ybuf, zup, zdn,
    load_sem, hand, send_sem, tok_recv, x_recv, up_recv, dn_recv,
    y_recv, zu_recv, zd_recv, dn_send, y_send, zu_send, zd_send,
):
    g, f, t = lax.axis_index("gr"), lax.axis_index("fs"), lax.axis_index("tp")
    z, y = f // Y, f % Y
    q = g * T + t
    rows = upw_v.shape[0]
    sub = rows // G
    unit = up_full.shape[1]
    dcols = dnw_v.shape[1]
    feat = part.shape[2]
    here = tok_full.shape[1]
    slab = here // E
    batch = here // B
    per = G * T // Z
    pending = []

    def nth(i):
        value = 0 * z
        for zv in range(Z):
            order = sorted(range(Z), key=lambda zd: (-abs(zd - zv), zd))
            for o in range(Z):
                value = jnp.where((z == zv) & (i == o), order[o], value)
        return value

    def fresh():
        assert len(pending) < send_count
        return send_sem.at[len(pending)]

    def send(src, dst, rsem, dev, cond=None):
        copy = pltpu.make_async_remote_copy(
            src_ref=src, dst_ref=dst, send_sem=fresh(), recv_sem=rsem, device_id=dev, device_id_type=MESH
        )
        if cond is None:
            copy.start()
        else:
            pl.when(cond)(copy.start)
        pending.append((cond, copy))

    def arrived(ref, sem, cond=None):
        wait = pltpu.make_async_copy(ref, ref, sem).wait
        if cond is None:
            wait()
        else:
            pl.when(cond)(wait)

    def tok(c, e):
        return tok_full.at[c, pl.ds(e * batch, batch)]

    loads = []
    for e in range(B):
        loads.append(pltpu.make_async_copy(tok_ref.at[pl.ds(e * batch, batch)], tok(f, e), tok_recv.at[f, e]))
    loads.append(pltpu.make_async_copy(gain_ref, gain_v, load_sem.at[0]))
    for h in range(G):
        r = pl.ds(h * sub, sub)
        loads.append(pltpu.make_async_copy(upw_ref.at[r], upw_v.at[r], load_sem.at[1 + h]))
    loads.append(pltpu.make_async_copy(dnw_ref, dnw_v, load_sem.at[1 + G]))

    barrier = pltpu.get_barrier_semaphore()
    below, above = z > 0, z < Z - 1

    def tell(sem, dev):
        pl.semaphore_signal(sem, inc=1, device_id=dev, device_id_type=MESH)

    def tell_across(sem):
        for o in range(1, Y):
            tell(sem, (g, z * Y + (y + o) % Y, t))

    def tell_chip(sem):
        for o in range(1, T):
            tell(sem, (g, f, (t + o) % T))

    for at in list(range(B, B + 1 + G)) + list(range(B)) + [B + 1 + G]:
        loads[at].start()
    for o in range(1, Z):
        tell(barrier, (g, ((z + o) % Z) * Y + y, t))
    for o in range(1, G):
        tell(barrier, ((g + o) % G, f, t))
    tell_across(barrier)
    tell_chip(barrier)

    loads[B].wait()
    wide_gain = jnp.broadcast_to(gain_v[...], (128, rows))
    gain_col[...] = wide_gain.T

    step = chunks(sub, 32)

    def convert_up(h):
        @pl.loop(0, sub // step)
        def _(i):
            r = pl.ds(pl.multiple_of(h * sub + i * step, step), step)
            column = gain_col[r, 0:1]
            for j in range(k):
                up_bf[j, r, :] = (column * upw_v[r, pl.ds(j * unit, unit)]).astype(jnp.bfloat16)

    bit = sub // S

    def piece(c, h, s):
        return up_full.at[pl.ds(pl.multiple_of(c * rows + h * sub + s * bit, bit), bit)]

    def half(j, h, s):
        return up_bf.at[j, pl.ds(pl.multiple_of(h * sub + s * bit, bit), bit)]

    def share_tokens(e):
        loads[e].wait()
        own = tok(f, e)
        for o in range(1, Y):
            send(own, own, tok_recv.at[f, e], (g, z * Y + (y + o) % Y, t))
        send(own, own, tok_recv.at[f, e], (g, f + Y, t), above)
        send(own, own, tok_recv.at[f, e], (g, f - Y, t), below)

    def xpart(og, j, s):
        return xbuf.at[og, j, pl.ds(s * bit, bit)]

    def start_exchange():
        for oh in range(1, G):
            h = (g + oh) % G
            for s in range(S):
                for j in range(k):
                    send(half(j, h, s), xpart(G - oh, j, s), x_recv.at[j, G - oh, s], (h, f, t))

    relay_core = f % T

    def to_owner(j, s, source_q, src):
        owner = source_q * k + j
        local = pltpu.make_async_copy(src, piece(f, g, s), up_recv.at[f, g, s])
        stays = (owner == f) & (relay_core == t)
        pl.when(stays)(local.start)
        send(src, piece(f, g, s), up_recv.at[f, g, s], (g, owner, relay_core), jnp.logical_not(stays))

    def start_owned():
        for s in range(S):
            for j in range(k):
                to_owner(j, s, q, half(j, g, s))

    deep = dnw_v.shape[0]
    drows = deep // C

    def dn_block(index, i):
        return dn_full.at[pl.ds(i * drows, drows), pl.ds(pl.multiple_of(index * dcols, dcols), dcols)]

    dstep = chunks(deep, 64)

    def start_down():
        loads[B + 1 + G].wait()

        @pl.loop(0, deep // dstep)
        def _(i):
            r = pl.ds(pl.multiple_of(i * dstep, dstep), dstep)
            dn_full[r, pl.ds(pl.multiple_of(q * dcols, dcols), dcols)] = dnw_v[r, :].astype(jnp.bfloat16)

        for i in range(C):
            for o in range(1, T):
                send(dn_block(q, i), dn_block(q, i), dn_recv.at[q, i], (g, f, (t + o) % T))


    def down_across(first, last, near=None):
        cond = None if near is None else ((nth(0) == q // per) == near)
        for i in range(first, last):
            for o in range(1, G):
                send(dn_block(q, i), dn_block(q, i), dn_recv.at[q, i], ((g + o) % G, f, t), cond)

    def relay_direct(c, s, cond):
        ok = (c % T == t) & cond
        arrived(piece(c, g, s), up_recv.at[c, g, s], ok)
        for o in range(1, G):
            send(piece(c, g, s), piece(c, g, s), up_recv.at[c, g, s], ((g + o) % G, f, t), ok)
        for o in range(1, T):
            send(piece(c, g, s), piece(c, g, s), up_recv.at[c, g, s], (g, f, (t + o) % T), ok)

    def relay_far(c, s, cond):
        ok = (c % T == t) & cond
        for oh in range(1, G):
            h = (g + oh) % G
            arrived(piece(c, h, s), up_recv.at[c, h, s], ok)
            for o in range(1, T):
                send(piece(c, h, s), piece(c, h, s), up_recv.at[c, h, s], (g, f, (t + o) % T), ok)

    def on_tokens(c, e, cond, up, down):
        arrived(tok(c, e), tok_recv.at[c, e], cond)
        if up is not None:
            send(tok(c, e), tok(c, e), tok_recv.at[c, e], (g, f + Y, t), up)
        if down is not None:
            send(tok(c, e), tok(c, e), tok_recv.at[c, e], (g, f - Y, t), down)
        for o in range(1, Y):
            send(tok(c, e), tok(c, e), tok_recv.at[c, e], (g, z * Y + (y + o) % Y, t), cond)

    def from_exchange(j, s):
        for og in range(1, G):
            arrived(xpart(og, j, s), x_recv.at[j, og, s])
            to_owner(j, s, ((g + og) % G) * T + t, xpart(og, j, s))

    def pieces_at(s):
        if s == 0:
            return [(z * Y + (y + o) % Y, True) for o in range(Y)]
        lower, upper = z - s >= 0, z + s < Z
        zl, zu = jnp.maximum(z - s, 0), jnp.minimum(z + s, Z - 1)
        found = []
        for o in range(Y):
            found.append((zl * Y + (y + o) % Y, lower))
            found.append((zu * Y + (y + o) % Y, upper))
        return found

    def tokens_at(s, e):
        lower, upper = z - s >= 0, z + s < Z
        zl, zu = jnp.maximum(z - s, 0), jnp.minimum(z + s, Z - 1)
        on_tokens(zl * Y + y, e, lower, lower & above, None)
        on_tokens(zu * Y + y, e, upper, None, upper & below)

    def greet_rest():
        pl.semaphore_wait(hand.at[0], (Y - 1) + (T - 1))
        tell_chip(hand.at[1])
        if T > 1:
            pl.semaphore_wait(hand.at[1], T - 1)

    def on_pieces(far, s, relay):
        for c, cond in pieces_at(far):
            relay(c, s, cond)

    for copy in loads[B + 1:B + 1 + G]:
        copy.wait()
    for h in range(G):
        convert_up(h)
    pl.semaphore_wait(barrier, (Z - 1) + (G - 1) + (Y - 1) + (T - 1))
    tell_across(hand.at[0])
    tell_chip(hand.at[0])
    for step_name in plan(Z, B, k, S, C):
        kind, *at = step_name
        {
            "share": share_tokens, "exchange": start_exchange, "greet": greet_rest,
            "owned": start_owned, "pass": from_exchange, "tokens": tokens_at, "down": start_down,
            "down across": down_across,
            "direct": lambda far, s: on_pieces(far, s, relay_direct), "far": lambda far, s: on_pieces(far, s, relay_far),
        }[kind](*at)

    @pl.loop(0, n)
    def _(c):
        for h in range(G):
            for s in range(S):
                arrived(piece(c, h, s), up_recv.at[c, h, s], c % T != t)

    width = n * tok_full.shape[2]

    def span(e):
        return pl.ds(pl.multiple_of(e * slab, slab), slab)

    def layer1(e):
        r = span(e)
        @pl.when(e % (E // B) == 0)
        def _():
            for zc in range(Z):
                for o in range(1, Y):
                    c = zc * Y + (y + o) % Y
                    at = e // (E // B)
                    rows_in = pl.ds(pl.multiple_of(at * batch, batch), batch)
                    arrived(tok_full.at[c, rows_in], tok_recv.at[c, at])

        blocks = [tok_full[c, r, :] for c in range(n)]
        squares = None
        for block in blocks:
            wide = block.astype(jnp.float32)
            total = jnp.sum(wide * wide, axis=1, keepdims=True)
            squares = total if squares is None else squares + total
        scale = lax.rsqrt(squares / width + epsilon)
        raw = jnp.dot(jnp.concatenate(blocks, axis=1), up_full[...], preferred_element_type=jnp.float32)
        hidden[r, :] = jnp.square(jnp.maximum(raw * scale, 0.0)).astype(jnp.bfloat16)

    def cross_copy(zd, o, e):
        y2 = (y + o) % Y
        return pltpu.make_async_remote_copy(
            src_ref=part.at[zd * Y + y2, span(e)], dst_ref=ybuf.at[zd, Y - o, span(e)], send_sem=y_send.at[zd, o, e],
            recv_sem=y_recv.at[zd, Y - o, e], device_id=(g, z * Y + y2, t), device_id_type=MESH,
        )

    def line_copy(zd, e, up):
        c = zd * Y + y
        if up:
            return pltpu.make_async_remote_copy(
                src_ref=part.at[c, span(e)], dst_ref=zup.at[zd, span(e)], send_sem=zu_send.at[zd, e],
                recv_sem=zu_recv.at[zd, e], device_id=(g, f + Y, t), device_id_type=MESH,
            )
        return pltpu.make_async_remote_copy(
            src_ref=part.at[c, span(e)], dst_ref=zdn.at[zd, span(e)], send_sem=zd_send.at[zd, e],
            recv_sem=zd_recv.at[zd, e], device_id=(g, f - Y, t), device_id_type=MESH,
        )

    def layer2(i, e):
        r = span(e)
        zd = nth(i)
        cols = dn_full[:, pl.ds(pl.multiple_of(zd * (Y * feat), Y * feat), Y * feat)]
        whole = jnp.dot(hidden[r, :], cols, preferred_element_type=jnp.float32).astype(jnp.bfloat16)
        for y2 in range(Y):
            part[zd * Y + y2, r, :] = whole[:, y2 * feat:(y2 + 1) * feat]
        for o in range(1, Y):
            cross_copy(zd, o, e).start()

    rstep = chunks(slab, 32)
    fstep = chunks(slab, 128)

    def add_up(c, e, extras, final=False):
        size = fstep if final else rstep

        @pl.loop(0, slab // size)
        def _(i):
            r = pl.ds(pl.multiple_of(e * slab + i * size, size), size)
            total = part[c, r, :].astype(jnp.float32)
            for ref, base in extras:
                total = total + ref[pl.ds(pl.multiple_of(base + i * size, size), size), :].astype(jnp.float32)
            if final:
                mixed_ref[:, r] = total.T.astype(jnp.bfloat16)
            else:
                part[c, r, :] = total.astype(jnp.bfloat16)

    ends = [
        (jnp.bool_(True), False, False) if Z == 1 else (z == 0, False, True),
    ]
    if Z > 1:
        ends.append((z == Z - 1, True, False))
    if Z > 2:
        ends.append((below & above, True, True))

    def finish(e, low, high, crossed):
        for cond, has_low, has_high in ends:
            extras = list(crossed) + ([low] if has_low else []) + ([high] if has_high else [])

            @pl.when(cond)
            def _():
                add_up(z * Y + y, e, extras, True)

    def add_step(index):
        held = jnp.clip(index, 0, items - 1)
        zd, e = nth(held // E), held % E
        go = (index >= 0) & (index < items)
        going_up, going_down = go & (zd > z), go & (zd < z)
        c = zd * Y + y
        base = e * slab
        crossed = [(ybuf.at[zd, o], base) for o in range(1, Y)]
        low, high = (zup.at[zd], base), (zdn.at[zd], base)
        for o in range(1, Y):
            arrived(ybuf.at[zd, o, span(e)], y_recv.at[zd, o, e], go)
        arrived(zup.at[zd, span(e)], zu_recv.at[zd, e], go & (zd >= z) & below)
        arrived(zdn.at[zd, span(e)], zd_recv.at[zd, e], go & (zd <= z) & above)
        if crossed:
            pl.when((going_up & (z == 0)) | (going_down & (z == Z - 1)))(lambda: add_up(c, e, crossed))
        pl.when(going_up & below)(lambda: add_up(c, e, crossed + [low]))
        pl.when(going_down & above)(lambda: add_up(c, e, crossed + [high]))
        pl.when(going_up)(lambda: line_copy(zd, e, True).start())
        pl.when(going_down)(lambda: line_copy(zd, e, False).start())
        pl.when(go & (zd == z))(lambda: finish(e, low, high, crossed))

    def down_over(b, o, i):
        return pltpu.make_async_remote_copy(
            src_ref=dn_block(b, i), dst_ref=dn_block(b, i), send_sem=dn_send.at[b, o, i],
            recv_sem=dn_recv.at[b, i], device_id=(g, f, (t + o) % T), device_id_type=MESH,
        )

    def down_forward(i):
        zd = nth(i)
        for at in range(per):
            b = zd * per + at

            @pl.when((b // T != g) & (b % T == t))
            def _():
                for part_of in range(C):
                    arrived(dn_block(b, part_of), dn_recv.at[b, part_of])
                    for o in range(1, T):
                        down_over(b, o, part_of).start()

    def down_wait(i):
        zd = nth(i)
        for at in range(per):
            b = zd * per + at

            @pl.when(b % T != t)
            def _():
                for part_of in range(C):
                    arrived(dn_block(b, part_of), dn_recv.at[b, part_of])

    items = Z * E
    delay = LAG + jnp.where(below & above, INNER, 0)
    down_forward(0)

    @pl.loop(0, items + LAG + INNER)
    def _(stage):
        @pl.when(stage < items)
        def _():
            i, e = stage // E, stage % E
            pl.when(i == 0)(lambda: layer1(e))
            pl.when((e == E - 1) & (i < Z - 1))(lambda: down_forward(i + 1))
            pl.when(e == 0)(lambda: down_wait(i))
            layer2(i, e)

        add_step(stage - delay)

    for cond, copy in pending:
        if cond is None:
            copy.wait_send()
        else:
            pl.when(cond)(copy.wait_send)
    for e in range(E):
        for zd in range(Z):
            for o in range(1, Y):
                cross_copy(zd, o, e).wait_send()
            pl.when(zd > z)(line_copy(zd, e, True).wait_send)
            pl.when(zd < z)(line_copy(zd, e, False).wait_send)
    for b in range(G * T):
        for o in range(1, T):
            for i in range(C):
                pl.when((b // T != g) & (b % T == t))(down_over(b, o, i).wait_send)


def drain(cuts, mixed_in, up_in, dn_in, mixed_out, up_out, dn_out, sems):
    copies = []
    for at, (src, dst) in enumerate([(up_in, up_out), (dn_in, dn_out), (mixed_in, mixed_out)]):
        size = src.shape[0] // cuts
        for i in range(cuts):
            r = pl.ds(i * size, size)
            copies.append(pltpu.make_async_copy(src.at[r], dst.at[r], sems.at[at, i]))
    for copy in copies:
        copy.start()
    for copy in copies:
        copy.wait()


def shards(dims, tokens, norm_gain, up_weight, down_weight):
    G, n, T = dims
    Z, Y = line_shape(n)
    rows, cols = up_weight.shape
    here, w = tokens.shape
    deep, dcols = down_weight.shape
    unit = cols * G * T // n
    k = n // (G * T)
    E = 4 if here % 128 == 0 else 1
    B = E
    S, C, LAG, INNER = 1, 4, 2, 2
    width = rows * n
    feat = dcols * G * T // n
    sends = B * (Y + 1) + 2 * (Z - 1) * B * Y
    sends += k * (G - 1) * S + k * G * S + C * (T - 1) + 2 * C * (G - 1)
    sends += (2 * Z - 1) * Y * S * ((G - 1) + G * (T - 1))
    bf = jnp.bfloat16
    dma = pltpu.SemaphoreType.DMA
    vmem = pl.BlockSpec(memory_space=pltpu.VMEM)
    hbm = pl.BlockSpec(memory_space=pltpu.HBM)
    held = pl.pallas_call(
        functools.partial(kernel, G, n, T, Z, Y, k, E, B, S, C, LAG, INNER, sends),
        out_shape=(
            pltpu.VMEM((feat, here), bf),
            pltpu.VMEM((width, unit), bf),
            pltpu.VMEM((deep, dcols * G * T), bf),
        ),
        in_specs=[hbm] * 4,
        out_specs=(vmem, vmem, vmem),
        scratch_shapes=[
            pltpu.VMEM((rows, cols), jnp.float32),
            pltpu.VMEM((deep, dcols), jnp.float32),
            pltpu.VMEM((1, rows), jnp.float32),
            pltpu.VMEM((rows, 128), jnp.float32),
            pltpu.VMEM((k, rows, unit), bf),
            pltpu.VMEM((G, k, rows // G, unit), bf),
            pltpu.VMEM((n, here, w), bf),
            pltpu.VMEM((here, unit), bf),
            pltpu.VMEM((n, here, feat), bf),
            pltpu.VMEM((Z, Y, here, feat), bf),
            pltpu.VMEM((Z, here, feat), bf),
            pltpu.VMEM((Z, here, feat), bf),
            dma((G + 2,)), pltpu.SemaphoreType.REGULAR((2,)), dma((sends,)),
            dma((n, B)), dma((k, G, S)), dma((n, G, S)), dma((G * T, C)),
            dma((Z, Y, E)), dma((Z, E)), dma((Z, E)), dma((G * T, T, C)), dma((Z, Y, E)), dma((Z, E)), dma((Z, E)),
        ],
        compiler_params=pltpu.CompilerParams(
            collective_id=0, has_side_effects=True, vmem_limit_bytes=52 * 1024 * 1024
        ),
    )(tokens, norm_gain[None, :], up_weight, down_weight)
    cuts = 4
    return pl.pallas_call(
        functools.partial(drain, cuts),
        out_shape=tuple(jax.ShapeDtypeStruct(x.shape, bf) for x in held),
        in_specs=[vmem] * 3,
        out_specs=(hbm,) * 3,
        scratch_shapes=[dma((3, cuts))],
        compiler_params=pltpu.CompilerParams(vmem_limit_bytes=12 * 1024 * 1024),
    )(*held)


def solution(mesh):
    dims = (mesh.shape["gr"], mesh.shape["fs"], mesh.shape["tp"])
    in_specs = (P(("gr", "tp"), "fs"), P("fs"), P("fs", ("gr", "tp")), P("fs", ("gr", "tp")))
    out_specs = (P("fs", ("gr", "tp")), P(None, "fs"), P("fs", None))
    return jax.shard_map(
        functools.partial(shards, dims), mesh=mesh, in_specs=in_specs, out_specs=out_specs, check_vma=False
    )
```

```python
import functools

import jax
import jax.numpy as jnp
from jax import lax
from jax.experimental import pallas as pl
from jax.experimental.pallas import tpu as pltpu
from jax.sharding import PartitionSpec as P

MESH = pl.DeviceIdType.MESH
epsilon = 1e-06


def line_shape(count):
    short = max(d for d in range(1, count + 1) if count % d == 0 and d * d <= count)
    return count // short, short


def chunks(total, size):
    return min(total, size)


def plan(Z, B, k, S, C):
    early = C // 2
    steps = [("exchange",)] + [("share", e) for e in range(B)] + [("down",), ("down across", 0, C, True), ("down across", 0, early, False)]
    steps += [("greet",), ("owned",)]
    steps += [("pass", j, s) for s in range(S) for j in range(k)]
    for far in range(Z - 1):
        steps += [("direct", far, s) for s in range(S)]
        if far + 2 == Z:
            steps += [("direct", Z - 1, s) for s in range(S)] + [("down across", early, C, False)]
        for e in range(B):
            steps += [("tokens", far + 1, e)]
            if far + 2 == Z:
                steps += [("far", at, s) for s in range(S) for at in range(e * Z // B, (e + 1) * Z // B)]
    return steps


def kernel(
    G, n, T, Z, Y, k, E, B, S, C, LAG, INNER, send_count,
    tok_ref, gain_ref, upw_ref, dnw_ref,
    mixed_ref, up_full, dn_full,
    upw_v, dnw_v, gain_v, gain_col, up_bf, xbuf, tok_full, hidden, part,
    ybuf, zup, zdn,
    load_sem, hand, send_sem, tok_recv, x_recv, up_recv, dn_recv,
    y_recv, zu_recv, zd_recv, dn_send, y_send, zu_send, zd_send,
):
    g, f, t = lax.axis_index("gr"), lax.axis_index("fs"), lax.axis_index("tp")
    z, y = f // Y, f % Y
    q = g * T + t
    rows = upw_v.shape[0]
    sub = rows // G
    unit = up_full.shape[1]
    dcols = dnw_v.shape[1]
    feat = part.shape[2]
    here = tok_full.shape[1]
    slab = here // E
    batch = here // B
    per = G * T // Z
    pending = []

    def nth(i):
        value = 0 * z
        for zv in range(Z):
            order = sorted(range(Z), key=lambda zd: (-abs(zd - zv), zd))
            for o in range(Z):
                value = jnp.where((z == zv) & (i == o), order[o], value)
        return value

    def fresh():
        assert len(pending) < send_count
        return send_sem.at[len(pending)]

    def send(src, dst, rsem, dev, cond=None):
        copy = pltpu.make_async_remote_copy(
            src_ref=src, dst_ref=dst, send_sem=fresh(), recv_sem=rsem, device_id=dev, device_id_type=MESH
        )
        if cond is None:
            copy.start()
        else:
            pl.when(cond)(copy.start)
        pending.append((cond, copy))

    def arrived(ref, sem, cond=None):
        wait = pltpu.make_async_copy(ref, ref, sem).wait
        if cond is None:
            wait()
        else:
            pl.when(cond)(wait)

    def tok(c, e):
        return tok_full.at[c, pl.ds(e * batch, batch)]

    loads = []
    for e in range(B):
        loads.append(pltpu.make_async_copy(tok_ref.at[pl.ds(e * batch, batch)], tok(f, e), tok_recv.at[f, e]))
    loads.append(pltpu.make_async_copy(gain_ref, gain_v, load_sem.at[0]))
    for h in range(G):
        r = pl.ds(h * sub, sub)
        loads.append(pltpu.make_async_copy(upw_ref.at[r], upw_v.at[r], load_sem.at[1 + h]))
    loads.append(pltpu.make_async_copy(dnw_ref, dnw_v, load_sem.at[1 + G]))

    barrier = pltpu.get_barrier_semaphore()
    below, above = z > 0, z < Z - 1

    def tell(sem, dev):
        pl.semaphore_signal(sem, inc=1, device_id=dev, device_id_type=MESH)

    def tell_across(sem):
        for o in range(1, Y):
            tell(sem, (g, z * Y + (y + o) % Y, t))

    def tell_chip(sem):
        for o in range(1, T):
            tell(sem, (g, f, (t + o) % T))

    for at in list(range(B, B + 1 + G)) + list(range(B)) + [B + 1 + G]:
        loads[at].start()
    for o in range(1, Z):
        tell(barrier, (g, ((z + o) % Z) * Y + y, t))
    for o in range(1, G):
        tell(barrier, ((g + o) % G, f, t))
    tell_across(barrier)
    tell_chip(barrier)

    loads[B].wait()
    wide_gain = jnp.broadcast_to(gain_v[...], (128, rows))
    gain_col[...] = wide_gain.T

    step = chunks(sub, 32)

    def convert_up(h):
        @pl.loop(0, sub // step)
        def _(i):
            r = pl.ds(pl.multiple_of(h * sub + i * step, step), step)
            column = gain_col[r, 0:1]
            for j in range(k):
                up_bf[j, r, :] = (column * upw_v[r, pl.ds(j * unit, unit)]).astype(jnp.bfloat16)

    bit = sub // S

    def piece(c, h, s):
        return up_full.at[pl.ds(pl.multiple_of(c * rows + h * sub + s * bit, bit), bit)]

    def half(j, h, s):
        return up_bf.at[j, pl.ds(pl.multiple_of(h * sub + s * bit, bit), bit)]

    def share_tokens(e):
        loads[e].wait()
        own = tok(f, e)
        for o in range(1, Y):
            send(own, own, tok_recv.at[f, e], (g, z * Y + (y + o) % Y, t))
        send(own, own, tok_recv.at[f, e], (g, f + Y, t), above)
        send(own, own, tok_recv.at[f, e], (g, f - Y, t), below)

    def xpart(og, j, s):
        return xbuf.at[og, j, pl.ds(s * bit, bit)]

    def start_exchange():
        for oh in range(1, G):
            h = (g + oh) % G
            for s in range(S):
                for j in range(k):
                    send(half(j, h, s), xpart(G - oh, j, s), x_recv.at[j, G - oh, s], (h, f, t))

    relay_core = f % T

    def to_owner(j, s, source_q, src):
        owner = source_q * k + j
        local = pltpu.make_async_copy(src, piece(f, g, s), up_recv.at[f, g, s])
        stays = (owner == f) & (relay_core == t)
        pl.when(stays)(local.start)
        send(src, piece(f, g, s), up_recv.at[f, g, s], (g, owner, relay_core), jnp.logical_not(stays))

    def start_owned():
        for s in range(S):
            for j in range(k):
                to_owner(j, s, q, half(j, g, s))

    deep = dnw_v.shape[0]
    drows = deep // C

    def dn_block(index, i):
        return dn_full.at[pl.ds(i * drows, drows), pl.ds(pl.multiple_of(index * dcols, dcols), dcols)]

    dstep = chunks(deep, 64)

    def start_down():
        loads[B + 1 + G].wait()

        @pl.loop(0, deep // dstep)
        def _(i):
            r = pl.ds(pl.multiple_of(i * dstep, dstep), dstep)
            dn_full[r, pl.ds(pl.multiple_of(q * dcols, dcols), dcols)] = dnw_v[r, :].astype(jnp.bfloat16)

        for i in range(C):
            for o in range(1, T):
                send(dn_block(q, i), dn_block(q, i), dn_recv.at[q, i], (g, f, (t + o) % T))


    def down_across(first, last, near=None):
        cond = None if near is None else ((nth(0) == q // per) == near)
        for i in range(first, last):
            for o in range(1, G):
                send(dn_block(q, i), dn_block(q, i), dn_recv.at[q, i], ((g + o) % G, f, t), cond)

    def relay_direct(c, s, cond):
        ok = (c % T == t) & cond
        arrived(piece(c, g, s), up_recv.at[c, g, s], ok)
        for o in range(1, G):
            send(piece(c, g, s), piece(c, g, s), up_recv.at[c, g, s], ((g + o) % G, f, t), ok)
        for o in range(1, T):
            send(piece(c, g, s), piece(c, g, s), up_recv.at[c, g, s], (g, f, (t + o) % T), ok)

    def relay_far(c, s, cond):
        ok = (c % T == t) & cond
        for oh in range(1, G):
            h = (g + oh) % G
            arrived(piece(c, h, s), up_recv.at[c, h, s], ok)
            for o in range(1, T):
                send(piece(c, h, s), piece(c, h, s), up_recv.at[c, h, s], (g, f, (t + o) % T), ok)

    def on_tokens(c, e, cond, up, down):
        arrived(tok(c, e), tok_recv.at[c, e], cond)
        if up is not None:
            send(tok(c, e), tok(c, e), tok_recv.at[c, e], (g, f + Y, t), up)
        if down is not None:
            send(tok(c, e), tok(c, e), tok_recv.at[c, e], (g, f - Y, t), down)
        for o in range(1, Y):
            send(tok(c, e), tok(c, e), tok_recv.at[c, e], (g, z * Y + (y + o) % Y, t), cond)

    def from_exchange(j, s):
        for og in range(1, G):
            arrived(xpart(og, j, s), x_recv.at[j, og, s])
            to_owner(j, s, ((g + og) % G) * T + t, xpart(og, j, s))

    def pieces_at(s):
        if s == 0:
            return [(z * Y + (y + o) % Y, True) for o in range(Y)]
        lower, upper = z - s >= 0, z + s < Z
        zl, zu = jnp.maximum(z - s, 0), jnp.minimum(z + s, Z - 1)
        found = []
        for o in range(Y):
            found.append((zl * Y + (y + o) % Y, lower))
            found.append((zu * Y + (y + o) % Y, upper))
        return found

    def tokens_at(s, e):
        lower, upper = z - s >= 0, z + s < Z
        zl, zu = jnp.maximum(z - s, 0), jnp.minimum(z + s, Z - 1)
        on_tokens(zl * Y + y, e, lower, lower & above, None)
        on_tokens(zu * Y + y, e, upper, None, upper & below)

    def greet_rest():
        pl.semaphore_wait(hand.at[0], (Y - 1) + (T - 1))
        tell_chip(hand.at[1])
        if T > 1:
            pl.semaphore_wait(hand.at[1], T - 1)

    def on_pieces(far, s, relay):
        for c, cond in pieces_at(far):
            relay(c, s, cond)

    for copy in loads[B + 1:B + 1 + G]:
        copy.wait()
    for h in range(G):
        convert_up(h)
    pl.semaphore_wait(barrier, (Z - 1) + (G - 1) + (Y - 1) + (T - 1))
    tell_across(hand.at[0])
    tell_chip(hand.at[0])
    for step_name in plan(Z, B, k, S, C):
        kind, *at = step_name
        {
            "share": share_tokens, "exchange": start_exchange, "greet": greet_rest,
            "owned": start_owned, "pass": from_exchange, "tokens": tokens_at, "down": start_down,
            "down across": down_across,
            "direct": lambda far, s: on_pieces(far, s, relay_direct), "far": lambda far, s: on_pieces(far, s, relay_far),
        }[kind](*at)

    @pl.loop(0, n)
    def _(c):
        for h in range(G):
            for s in range(S):
                arrived(piece(c, h, s), up_recv.at[c, h, s], c % T != t)

    width = n * tok_full.shape[2]

    def span(e):
        return pl.ds(pl.multiple_of(e * slab, slab), slab)

    def layer1(e):
        r = span(e)
        @pl.when(e % (E // B) == 0)
        def _():
            for zc in range(Z):
                for o in range(1, Y):
                    c = zc * Y + (y + o) % Y
                    at = e // (E // B)
                    rows_in = pl.ds(pl.multiple_of(at * batch, batch), batch)
                    arrived(tok_full.at[c, rows_in], tok_recv.at[c, at])

        blocks = [tok_full[c, r, :] for c in range(n)]
        squares = None
        for block in blocks:
            wide = block.astype(jnp.float32)
            total = jnp.sum(wide * wide, axis=1, keepdims=True)
            squares = total if squares is None else squares + total
        scale = lax.rsqrt(squares / width + epsilon)
        raw = jnp.dot(jnp.concatenate(blocks, axis=1), up_full[...], preferred_element_type=jnp.float32)
        hidden[r, :] = jnp.square(jnp.maximum(raw * scale, 0.0)).astype(jnp.bfloat16)

    def cross_copy(zd, o, e):
        y2 = (y + o) % Y
        return pltpu.make_async_remote_copy(
            src_ref=part.at[zd * Y + y2, span(e)], dst_ref=ybuf.at[zd, Y - o, span(e)], send_sem=y_send.at[zd, o, e],
            recv_sem=y_recv.at[zd, Y - o, e], device_id=(g, z * Y + y2, t), device_id_type=MESH,
        )

    def line_copy(zd, e, up):
        c = zd * Y + y
        if up:
            return pltpu.make_async_remote_copy(
                src_ref=part.at[c, span(e)], dst_ref=zup.at[zd, span(e)], send_sem=zu_send.at[zd, e],
                recv_sem=zu_recv.at[zd, e], device_id=(g, f + Y, t), device_id_type=MESH,
            )
        return pltpu.make_async_remote_copy(
            src_ref=part.at[c, span(e)], dst_ref=zdn.at[zd, span(e)], send_sem=zd_send.at[zd, e],
            recv_sem=zd_recv.at[zd, e], device_id=(g, f - Y, t), device_id_type=MESH,
        )

    def layer2(i, e):
        r = span(e)
        zd = nth(i)
        cols = dn_full[:, pl.ds(pl.multiple_of(zd * (Y * feat), Y * feat), Y * feat)]
        whole = jnp.dot(hidden[r, :], cols, preferred_element_type=jnp.float32).astype(jnp.bfloat16)
        for y2 in range(Y):
            part[zd * Y + y2, r, :] = whole[:, y2 * feat:(y2 + 1) * feat]
        for o in range(1, Y):
            cross_copy(zd, o, e).start()

    rstep = chunks(slab, 64)
    fstep = chunks(slab, 128)

    def add_up(c, e, extras, final=False):
        size = fstep if final else rstep

        @pl.loop(0, slab // size)
        def _(i):
            r = pl.ds(pl.multiple_of(e * slab + i * size, size), size)
            total = part[c, r, :].astype(jnp.float32)
            for ref, base in extras:
                total = total + ref[pl.ds(pl.multiple_of(base + i * size, size), size), :].astype(jnp.float32)
            if final:
                mixed_ref[:, r] = total.T.astype(jnp.bfloat16)
            else:
                part[c, r, :] = total.astype(jnp.bfloat16)

    ends = [
        (jnp.bool_(True), False, False) if Z == 1 else (z == 0, False, True),
    ]
    if Z > 1:
        ends.append((z == Z - 1, True, False))
    if Z > 2:
        ends.append((below & above, True, True))

    def finish(e, low, high, crossed):
        for cond, has_low, has_high in ends:
            extras = list(crossed) + ([low] if has_low else []) + ([high] if has_high else [])

            @pl.when(cond)
            def _():
                add_up(z * Y + y, e, extras, True)

    def add_step(index):
        held = jnp.clip(index, 0, items - 1)
        zd, e = nth(held // E), held % E
        go = (index >= 0) & (index < items)
        going_up, going_down = go & (zd > z), go & (zd < z)
        c = zd * Y + y
        base = e * slab
        crossed = [(ybuf.at[zd, o], base) for o in range(1, Y)]
        low, high = (zup.at[zd], base), (zdn.at[zd], base)
        for o in range(1, Y):
            arrived(ybuf.at[zd, o, span(e)], y_recv.at[zd, o, e], go)
        arrived(zup.at[zd, span(e)], zu_recv.at[zd, e], go & (zd >= z) & below)
        arrived(zdn.at[zd, span(e)], zd_recv.at[zd, e], go & (zd <= z) & above)
        if crossed:
            pl.when((going_up & (z == 0)) | (going_down & (z == Z - 1)))(lambda: add_up(c, e, crossed))
        pl.when(going_up & below)(lambda: add_up(c, e, crossed + [low]))
        pl.when(going_down & above)(lambda: add_up(c, e, crossed + [high]))
        pl.when(going_up)(lambda: line_copy(zd, e, True).start())
        pl.when(going_down)(lambda: line_copy(zd, e, False).start())
        pl.when(go & (zd == z))(lambda: finish(e, low, high, crossed))

    def down_over(b, o, i):
        return pltpu.make_async_remote_copy(
            src_ref=dn_block(b, i), dst_ref=dn_block(b, i), send_sem=dn_send.at[b, o, i],
            recv_sem=dn_recv.at[b, i], device_id=(g, f, (t + o) % T), device_id_type=MESH,
        )

    def down_forward(i):
        zd = nth(i)
        for at in range(per):
            b = zd * per + at

            @pl.when((b // T != g) & (b % T == t))
            def _():
                for part_of in range(C):
                    arrived(dn_block(b, part_of), dn_recv.at[b, part_of])
                    for o in range(1, T):
                        down_over(b, o, part_of).start()

    def down_wait(i):
        zd = nth(i)
        for at in range(per):
            b = zd * per + at

            @pl.when(b % T != t)
            def _():
                for part_of in range(C):
                    arrived(dn_block(b, part_of), dn_recv.at[b, part_of])

    items = Z * E
    delay = LAG + jnp.where(below & above, INNER, 0)
    down_forward(0)

    @pl.loop(0, items + LAG + INNER)
    def _(stage):
        @pl.when(stage < items)
        def _():
            i, e = stage // E, stage % E
            pl.when(i == 0)(lambda: layer1(e))
            pl.when((e == E - 1) & (i < Z - 1))(lambda: down_forward(i + 1))
            pl.when(e == 0)(lambda: down_wait(i))
            layer2(i, e)

        add_step(stage - delay)

    for cond, copy in pending:
        if cond is None:
            copy.wait_send()
        else:
            pl.when(cond)(copy.wait_send)
    for e in range(E):
        for zd in range(Z):
            for o in range(1, Y):
                cross_copy(zd, o, e).wait_send()
            pl.when(zd > z)(line_copy(zd, e, True).wait_send)
            pl.when(zd < z)(line_copy(zd, e, False).wait_send)
    for b in range(G * T):
        for o in range(1, T):
            for i in range(C):
                pl.when((b // T != g) & (b % T == t))(down_over(b, o, i).wait_send)


def drain(cuts, mixed_in, up_in, dn_in, mixed_out, up_out, dn_out, sems):
    copies = []
    for at, (src, dst) in enumerate([(up_in, up_out), (dn_in, dn_out), (mixed_in, mixed_out)]):
        size = src.shape[0] // cuts
        for i in range(cuts):
            r = pl.ds(i * size, size)
            copies.append(pltpu.make_async_copy(src.at[r], dst.at[r], sems.at[at, i]))
    for copy in copies:
        copy.start()
    for copy in copies:
        copy.wait()


def shards(dims, tokens, norm_gain, up_weight, down_weight):
    G, n, T = dims
    Z, Y = line_shape(n)
    rows, cols = up_weight.shape
    here, w = tokens.shape
    deep, dcols = down_weight.shape
    unit = cols * G * T // n
    k = n // (G * T)
    E = 4 if here % 128 == 0 else 1
    B = E
    S, C, LAG, INNER = 1, 4, 2, 2
    width = rows * n
    feat = dcols * G * T // n
    sends = B * (Y + 1) + 2 * (Z - 1) * B * Y
    sends += k * (G - 1) * S + k * G * S + C * (T - 1) + 2 * C * (G - 1)
    sends += (2 * Z - 1) * Y * S * ((G - 1) + G * (T - 1))
    bf = jnp.bfloat16
    dma = pltpu.SemaphoreType.DMA
    vmem = pl.BlockSpec(memory_space=pltpu.VMEM)
    hbm = pl.BlockSpec(memory_space=pltpu.HBM)
    held = pl.pallas_call(
        functools.partial(kernel, G, n, T, Z, Y, k, E, B, S, C, LAG, INNER, sends),
        out_shape=(
            pltpu.VMEM((feat, here), bf),
            pltpu.VMEM((width, unit), bf),
            pltpu.VMEM((deep, dcols * G * T), bf),
        ),
        in_specs=[hbm] * 4,
        out_specs=(vmem, vmem, vmem),
        scratch_shapes=[
            pltpu.VMEM((rows, cols), jnp.float32),
            pltpu.VMEM((deep, dcols), jnp.float32),
            pltpu.VMEM((1, rows), jnp.float32),
            pltpu.VMEM((rows, 128), jnp.float32),
            pltpu.VMEM((k, rows, unit), bf),
            pltpu.VMEM((G, k, rows // G, unit), bf),
            pltpu.VMEM((n, here, w), bf),
            pltpu.VMEM((here, unit), bf),
            pltpu.VMEM((n, here, feat), bf),
            pltpu.VMEM((Z, Y, here, feat), bf),
            pltpu.VMEM((Z, here, feat), bf),
            pltpu.VMEM((Z, here, feat), bf),
            dma((G + 2,)), pltpu.SemaphoreType.REGULAR((2,)), dma((sends,)),
            dma((n, B)), dma((k, G, S)), dma((n, G, S)), dma((G * T, C)),
            dma((Z, Y, E)), dma((Z, E)), dma((Z, E)), dma((G * T, T, C)), dma((Z, Y, E)), dma((Z, E)), dma((Z, E)),
        ],
        compiler_params=pltpu.CompilerParams(
            collective_id=0, has_side_effects=True, vmem_limit_bytes=52 * 1024 * 1024
        ),
    )(tokens, norm_gain[None, :], up_weight, down_weight)
    cuts = 4
    return pl.pallas_call(
        functools.partial(drain, cuts),
        out_shape=tuple(jax.ShapeDtypeStruct(x.shape, bf) for x in held),
        in_specs=[vmem] * 3,
        out_specs=(hbm,) * 3,
        scratch_shapes=[dma((3, cuts))],
        compiler_params=pltpu.CompilerParams(vmem_limit_bytes=12 * 1024 * 1024),
    )(*held)


def solution(mesh):
    dims = (mesh.shape["gr"], mesh.shape["fs"], mesh.shape["tp"])
    in_specs = (P(("gr", "tp"), "fs"), P("fs"), P("fs", ("gr", "tp")), P("fs", ("gr", "tp")))
    out_specs = (P("fs", ("gr", "tp")), P(None, "fs"), P("fs", None))
    return jax.shard_map(
        functools.partial(shards, dims), mesh=mesh, in_specs=in_specs, out_specs=out_specs, check_vma=False
    )
```
